32 devices in a mesh: ep: 32 (over z, y, x, core).
Axes of the slice: x: 2, y: 2, z: 4, core: 2. Of those that a mesh axis runs over, the one named last changes fastest.
Arguments:
- latest_embeddings: bfloat16 [512, 2048], P('ep'), may hold values from -6 to 6
- prior_memory_grids: float32 [512, 32, 4096], P('ep'), may hold values from -1.75 to 1.75
- earlier_rescale_gain: float32 [2048], replicated, may hold values from 0.1 to 1.9
- query_map: bfloat16 [2048, 2048], P(None, 'ep'), may hold values from -0.125 to 0.125
- lookup_map: bfloat16 [2048, 2048], P(None, 'ep'), may hold values from -0.125 to 0.125
- content_map: bfloat16 [2048, 2048], P(None, 'ep'), may hold values from -0.125 to 0.125
- forget_lower_map: bfloat16 [2048, 64], replicated, may hold values from -0.125 to 0.125
- forget_upper_map: bfloat16 [64, 2048], replicated, may hold values from -0.75 to 0.75
- forget_shift: float32 [2048], replicated, may hold values from -3 to 3
- adapt_lower_map: bfloat16 [2048, 64], replicated, may hold values from -0.125 to 0.125
- adapt_upper_map: bfloat16 [64, 2048], replicated, may hold values from -0.75 to 0.75
- adapt_shift: float32 [2048], replicated, may hold values from -2 to 2
- erase_lookup_gains: float32 [2048], replicated, may hold values from 0.1 to 1.9
- substitute_lookup_gains: float32 [2048], replicated, may hold values from 0.1 to 1.9
- present_extra_gains: float32 [2048], replicated, may hold values from -1.75 to 1.75
- attender_rescale_gain: float32 [2048], replicated, may hold values from 0.1 to 1.9
- result_map: bfloat16 [2048, 2048], P(None, 'ep'), may hold values from -0.125 to 0.125
- later_rescale_gain: float32 [2048], replicated, may hold values from 0.1 to 1.9
- specialist_switch_maps: bfloat16 [32, 2048, 512], P('ep'), may hold values from -0.125 to 0.125
- specialist_widen_maps: bfloat16 [32, 2048, 512], P('ep'), may hold values from -0.125 to 0.125
- specialist_shrink_maps: bfloat16 [32, 512, 2048], P('ep'), may hold values from -0.25 to 0.25
- picked_specialists: int32 [512, 6], P('ep'), may hold values from 0 to 31, as said below
- specialist_picked_shares: float32 [512, 6], P('ep'), may hold values from 0.02 to 0.5
Outputs:
- new_hidden: bfloat16 [512, 2048], P('ep')
- new_state: float32 [512, 32, 4096], P('ep')
The draws below stay inside these ranges and needn't reach their ends.
Inputs may be any that keep to these rules, and one draw needn't show every extreme that they name: `picked_specialists`: each row names 6 different experts of one group; a group is a run of 8 consecutive expert numbers. The rows of one device use exactly two groups, one of them for half of the device's rows rounded up and the other for the rest. No expert is named by more than 6 rows of one device, and on every device some expert is named by exactly 6.
All inputs are finite; a program needn't handle non-finite values.
Results may differ from the reference program's by a relative error of at most 0.011.
Values may be sent and summed in bfloat16 or wider, within the bound.
No kernel may reach another device: no remote copies, remote signals or barrier semaphores. Data moves between devices by JAX's collectives and lax.ppermute only.
A program may use at most 256 MiB of HBM per device.

```python
import math
import jax
import jax.numpy as jnp
from jax import lax

EMBED_WIDTH = 2048
CHANNEL_COUNT = 64
ATTENDER_COUNT = 32
LR = 64
FE = 512
GROUPS = 4
TOP = 6
EXPERTS = 32
SEQ_DEV = 16
SEQS = 512
CAP = 6
N_EP = 32


def draw_picked_specialists(key, part):
    group_size = EXPERTS // GROUPS
    half_rows = (SEQ_DEV + 1) // 2

    def one_device(device):
        base = jax.random.fold_in(jax.random.fold_in(key, 17), device)
        subkeys = jax.random.split(base, 5)
        ranking = jax.random.permutation(subkeys[0], SEQ_DEV)
        first_group = jax.random.randint(subkeys[1], (), 0, GROUPS)
        other_group = (first_group + 1 + jax.random.randint(subkeys[2], (), 0, GROUPS - 1)) % GROUPS
        leading = ranking < half_rows
        group_ids = jnp.where(leading, first_group, other_group)
        within_group = jnp.where(leading, ranking, ranking - half_rows)
        order_first = jax.random.permutation(subkeys[3], group_size)
        order_other = jax.random.permutation(subkeys[4], group_size)
        positions = (within_group[:, None] * TOP + jnp.arange(TOP)[None, :]) % group_size
        chosen = jnp.where(leading[:, None], order_first[positions], order_other[positions])
        return (group_ids[:, None] * group_size + chosen).astype(jnp.int32)
    blocks = jax.vmap(one_device)(jnp.arange(N_EP))
    return blocks.reshape(SEQ_DEV * N_EP, TOP)


def steps_of(own_key, shape, shards, low, largest):
    level = 1.0
    for axis_at, blocks in shards:
        heights = jax.random.uniform(jax.random.fold_in(jax.random.fold_in(own_key, 6), axis_at), (blocks,), jnp.float32, low / len(shards), largest / len(shards))
        level = level * jnp.repeat(jnp.exp(heights), shape[axis_at] // blocks).reshape((-1,) + (1,) * (len(shape) - 1 - axis_at))
    return level


def bell_draw(own_key, shape, spread, reach, shards=(), kind=jnp.bfloat16):
    drawn = spread * jax.random.normal(own_key, shape, jnp.float32)
    if shards:
        drawn = drawn * steps_of(own_key, shape, shards, -0.22, 0.18)
    return jnp.clip(drawn, -reach, reach).astype(kind)


def setup_inputs(seed: int = 0) -> dict:
    arg_keys = jax.random.split(jax.random.key(seed), 24)
    latest_embeddings = bell_draw(arg_keys[0], (SEQS, EMBED_WIDTH), 1.0, 6.0, ((0, 32),))
    prior_memory_grids = bell_draw(arg_keys[1], (SEQS, ATTENDER_COUNT, CHANNEL_COUNT * CHANNEL_COUNT), 0.3, 1.75, ((0, 32),), jnp.float32)
    earlier_rescale_gain = jnp.clip(1.0 + 0.18 * jax.random.normal(arg_keys[2], (EMBED_WIDTH,), jnp.float32), 0.1, 1.9)
    query_map = bell_draw(arg_keys[3], (EMBED_WIDTH, EMBED_WIDTH), EMBED_WIDTH ** -0.5, 0.125, ((1, 32),))
    lookup_map = bell_draw(arg_keys[4], (EMBED_WIDTH, EMBED_WIDTH), EMBED_WIDTH ** -0.5, 0.125, ((1, 32),))
    content_map = bell_draw(arg_keys[5], (EMBED_WIDTH, EMBED_WIDTH), EMBED_WIDTH ** -0.5, 0.125, ((1, 32),))
    forget_lower_map = bell_draw(arg_keys[6], (EMBED_WIDTH, LR), EMBED_WIDTH ** -0.5, 0.125)
    forget_upper_map = bell_draw(arg_keys[7], (LR, EMBED_WIDTH), LR ** -0.5, 0.75)
    forget_shift = jnp.clip(jax.random.uniform(arg_keys[8], (EMBED_WIDTH,), jnp.float32, -3.0, 3.0), -3.0, 3.0)
    adapt_lower_map = bell_draw(arg_keys[9], (EMBED_WIDTH, LR), EMBED_WIDTH ** -0.5, 0.125)
    adapt_upper_map = bell_draw(arg_keys[10], (LR, EMBED_WIDTH), LR ** -0.5, 0.75)
    adapt_shift = jnp.clip(jax.random.uniform(arg_keys[11], (EMBED_WIDTH,), jnp.float32, -2.0, 2.0), -2.0, 2.0)
    erase_lookup_gains = jnp.clip(1.0 + 0.18 * jax.random.normal(arg_keys[12], (EMBED_WIDTH,), jnp.float32), 0.1, 1.9)
    substitute_lookup_gains = jnp.clip(1.0 + 0.18 * jax.random.normal(arg_keys[13], (EMBED_WIDTH,), jnp.float32), 0.1, 1.9)
    present_extra_gains = bell_draw(arg_keys[14], (EMBED_WIDTH,), 0.3, 1.75, (), jnp.float32)
    attender_rescale_gain = jnp.clip(1.0 + 0.18 * jax.random.normal(arg_keys[15], (EMBED_WIDTH,), jnp.float32), 0.1, 1.9)
    result_map = bell_draw(arg_keys[16], (EMBED_WIDTH, EMBED_WIDTH), EMBED_WIDTH ** -0.5, 0.125, ((1, 32),))
    later_rescale_gain = jnp.clip(1.0 + 0.18 * jax.random.normal(arg_keys[17], (EMBED_WIDTH,), jnp.float32), 0.1, 1.9)
    specialist_switch_maps = bell_draw(arg_keys[18], (EXPERTS, EMBED_WIDTH, FE), EMBED_WIDTH ** -0.5, 0.125, ((0, 32),))
    specialist_widen_maps = bell_draw(arg_keys[19], (EXPERTS, EMBED_WIDTH, FE), EMBED_WIDTH ** -0.5, 0.125, ((0, 32),))
    specialist_shrink_maps = bell_draw(arg_keys[20], (EXPERTS, FE, EMBED_WIDTH), FE ** -0.5, 0.25, ((0, 32),))
    picked_specialists = draw_picked_specialists(jax.random.fold_in(arg_keys[23], 71), 0)
    specialist_picked_shares = jnp.clip(jnp.exp(math.log(0.5) - 3.218876 * jax.random.uniform(arg_keys[22], (SEQS, TOP), jnp.float32) ** steps_of(arg_keys[22], (SEQS, TOP), ((0, 32),), -0.2, 0.2)), 0.02, 0.5)
    return dict(latest_embeddings=latest_embeddings, prior_memory_grids=prior_memory_grids, earlier_rescale_gain=earlier_rescale_gain, query_map=query_map, lookup_map=lookup_map, content_map=content_map, forget_lower_map=forget_lower_map, forget_upper_map=forget_upper_map, forget_shift=forget_shift, adapt_lower_map=adapt_lower_map, adapt_upper_map=adapt_upper_map, adapt_shift=adapt_shift, erase_lookup_gains=erase_lookup_gains, substitute_lookup_gains=substitute_lookup_gains, present_extra_gains=present_extra_gains, attender_rescale_gain=attender_rescale_gain, result_map=result_map, later_rescale_gain=later_rescale_gain, specialist_switch_maps=specialist_switch_maps, specialist_widen_maps=specialist_widen_maps, specialist_shrink_maps=specialist_shrink_maps, picked_specialists=picked_specialists, specialist_picked_shares=specialist_picked_shares)


norm_eps = 1e-06
group_eps = 0.00064
unit_eps = 1e-06

def rms_norm(rows_in, gain):
    values = rows_in.astype(jnp.float32)
    scale = lax.rsqrt(lax.optimization_barrier(jnp.mean(values * values, axis=-1, keepdims=True)) + norm_eps)
    return (values * scale * gain.astype(jnp.float32)).astype(jnp.bfloat16)

def memory_readout(query_signal, substitute_lookup, content_signals, forget_multiplier, adapt_speed, erase_signal, memory_grid, attender_rescale_gain, present_extra_gains):
    highest = lax.Precision.HIGHEST
    removed = jnp.einsum('bhij,bhj->bhi', memory_grid, erase_signal, precision=highest)
    memory_grid = memory_grid * forget_multiplier[:, :, None, :] - removed[..., None] * (erase_signal * adapt_speed)[:, :, None, :] + content_signals[..., None] * substitute_lookup[:, :, None, :]
    readout = jnp.einsum('bhij,bhj->bhi', memory_grid, query_signal, precision=highest)
    centered = readout - lax.optimization_barrier(jnp.mean(readout, axis=-1, keepdims=True))
    variance = lax.optimization_barrier(jnp.mean(centered * centered, axis=-1, keepdims=True))
    rescaled_result = centered * lax.rsqrt(variance + group_eps) * attender_rescale_gain
    present_extra = lax.optimization_barrier(jnp.sum(query_signal * substitute_lookup * present_extra_gains, axis=-1, keepdims=True)) * content_signals
    return (rescaled_result + present_extra, memory_grid)

def reference(latest_embeddings, prior_memory_grids, earlier_rescale_gain, query_map, lookup_map, content_map, forget_lower_map, forget_upper_map, forget_shift, adapt_lower_map, adapt_upper_map, adapt_shift, erase_lookup_gains, substitute_lookup_gains, present_extra_gains, attender_rescale_gain, result_map, later_rescale_gain, specialist_switch_maps, specialist_widen_maps, specialist_shrink_maps, picked_specialists, specialist_picked_shares):
    normed = rms_norm(latest_embeddings, earlier_rescale_gain)
    query_signal = jnp.dot(normed, query_map, preferred_element_type=jnp.float32).astype(jnp.bfloat16)
    key_rows = jnp.dot(normed, lookup_map, preferred_element_type=jnp.float32).astype(jnp.bfloat16)
    content_signals = jnp.dot(normed, content_map, preferred_element_type=jnp.float32).astype(jnp.bfloat16)
    decay_low = jnp.tanh(jnp.dot(normed, forget_lower_map, preferred_element_type=jnp.float32)).astype(jnp.bfloat16)
    forget_multiplier = jnp.exp(-math.exp(-0.5) * jax.nn.sigmoid(forget_shift + jnp.dot(decay_low, forget_upper_map, preferred_element_type=jnp.float32)))
    rate_low = jnp.dot(normed, adapt_lower_map, preferred_element_type=jnp.float32).astype(jnp.bfloat16)
    adapt_speed = jax.nn.sigmoid(adapt_shift + jnp.dot(rate_low, adapt_upper_map, preferred_element_type=jnp.float32))
    key_float = key_rows.astype(jnp.float32)
    erase_signal = (key_float * erase_lookup_gains).reshape(SEQS, ATTENDER_COUNT, CHANNEL_COUNT)
    erase_signal = erase_signal * lax.rsqrt(lax.optimization_barrier(jnp.sum(erase_signal * erase_signal, axis=-1, keepdims=True)) + unit_eps)
    substitute_lookup = key_float * (1.0 + (adapt_speed - 1.0) * substitute_lookup_gains)

    def blocked(array):
        return array.reshape(N_EP, SEQ_DEV, ATTENDER_COUNT, CHANNEL_COUNT)

    def one_block(block_entry_signal):
        return memory_readout(*block_entry_signal, attender_rescale_gain.reshape(ATTENDER_COUNT, CHANNEL_COUNT), present_extra_gains.reshape(ATTENDER_COUNT, CHANNEL_COUNT))
    mixed_parts, state_parts = lax.map(one_block, (blocked(query_signal.astype(jnp.float32)), blocked(substitute_lookup), blocked(content_signals.astype(jnp.float32)), blocked(forget_multiplier), blocked(adapt_speed), erase_signal.reshape(N_EP, SEQ_DEV, ATTENDER_COUNT, CHANNEL_COUNT), prior_memory_grids.reshape(N_EP, SEQ_DEV, ATTENDER_COUNT, CHANNEL_COUNT, CHANNEL_COUNT)))
    mixed = mixed_parts.reshape(SEQS, EMBED_WIDTH).astype(jnp.bfloat16)
    new_state = state_parts.reshape(SEQS, ATTENDER_COUNT, CHANNEL_COUNT * CHANNEL_COUNT)
    mixer_out = jnp.dot(mixed, result_map, preferred_element_type=jnp.float32).astype(jnp.bfloat16)
    residual = (latest_embeddings.astype(jnp.float32) + mixer_out.astype(jnp.float32)).astype(jnp.bfloat16)
    second = rms_norm(residual, later_rescale_gain)
    slot_count = N_EP * CAP
    flat_ids = picked_specialists.reshape(-1).astype(jnp.int32)

    def one_expert(block_entry_signal):
        expert_id, gate_w, up_w, down_w = block_entry_signal
        matched = flat_ids == expert_id
        ranking = jnp.argsort(jnp.where(matched, 0, 1).astype(jnp.int32), stable=True)[:slot_count].astype(jnp.int32)
        picked_rows = second[ranking // TOP]
        gate_proj = jnp.dot(picked_rows, gate_w, preferred_element_type=jnp.float32)
        up_proj = jnp.dot(picked_rows, up_w, preferred_element_type=jnp.float32)
        hidden_act = (jax.nn.silu(gate_proj) * up_proj).astype(jnp.bfloat16)
        results = jnp.dot(hidden_act, down_w, preferred_element_type=jnp.float32).astype(jnp.bfloat16)
        return (results, ranking, matched[ranking])
    outputs, rankings, is_valid = lax.map(one_expert, (jnp.arange(EXPERTS, dtype=jnp.int32), specialist_switch_maps, specialist_widen_maps, specialist_shrink_maps))
    coefficient = specialist_picked_shares.reshape(-1)[rankings] * is_valid.astype(specialist_picked_shares.dtype)
    contrib = (coefficient[..., None] * outputs.astype(specialist_picked_shares.dtype)).reshape(-1, EMBED_WIDTH)
    expert_sum = jnp.zeros((SEQS, EMBED_WIDTH), specialist_picked_shares.dtype).at[(rankings // TOP).reshape(-1)].add(contrib)
    new_hidden = (residual.astype(jnp.float32) + expert_sum).astype(jnp.bfloat16)
    return (new_hidden, new_state)
```

```python
import functools
import math

import jax
import jax.numpy as jnp
from jax import lax
from jax.experimental import pallas as pl
from jax.experimental.pallas import tpu as pltpu
from jax.sharding import PartitionSpec as P

GROUPS = 4


norm_eps = 1e-06
group_eps = 0.00064
unit_eps = 1e-06

f32 = jnp.float32
bf16 = jnp.bfloat16


def full(shape):
    return pl.BlockSpec(shape, lambda *_: (0,) * len(shape))


def rms_rows(values, gain):
    scale = lax.rsqrt(jnp.mean(values * values, axis=-1, keepdims=True) + norm_eps)
    return (values * scale * gain).astype(bf16)


def split_dot(values, selector):
    high = values.astype(bf16)
    low = (values - high.astype(f32)).astype(bf16)
    return jnp.dot(high, selector, preferred_element_type=f32) + jnp.dot(
        low, selector, preferred_element_type=f32
    )


def project_kernel(chips, where_ref, *refs):
    rows_refs, gain_ref, weight_ref, out_ref = refs[:-3], refs[-3], refs[-2], refs[-1]
    plane, place = where_ref[0], where_ref[1]
    for kp, rows_ref in enumerate(rows_refs):
        normed = rms_rows(rows_ref[...].astype(f32), gain_ref[...])
        result = jnp.dot(normed, weight_ref[...], preferred_element_type=f32).astype(bf16)
        seqs = result.shape[0] // GROUPS
        for kz in range(GROUPS):
            chip = (plane ^ kz) * chips + (place ^ kp)
            out_ref[pl.ds(pl.multiple_of(chip * seqs, seqs), seqs), :] = result[
                kz * seqs : (kz + 1) * seqs
            ]


def state_kernel(
    channel,
    key_ref,
    query_ref,
    value_ref,
    decay_ref,
    rate_ref,
    erase_ref,
    substitute_ref,
    extra_ref,
    attend_ref,
    state_ref,
    new_ref,
    mixed_ref,
    erase2,
    write2,
    replace2,
    query2,
    decay2,
    readout,
):
    step = pl.program_id(0)
    seqs, heads, width = state_ref.shape
    rows = seqs * heads
    span = 256

    def flat(x):
        return x.astype(f32).reshape(rows, channel)

    def twice(x):
        return jnp.concatenate([x, x], axis=-1)

    @pl.when(step == 0)
    def _():
        key = flat(key_ref[...])
        rate = flat(rate_ref[...])
        erase = (key.reshape(seqs, heads, channel) * erase_ref[...][None]).reshape(rows, channel)
        erase = erase * lax.rsqrt(jnp.sum(erase * erase, axis=-1, keepdims=True) + unit_eps)
        gain = jnp.broadcast_to(substitute_ref[...][None], (seqs, heads, channel)).reshape(
            rows, channel
        )
        replace = key * (1.0 + (rate - 1.0) * gain)
        erase2[...] = twice(erase)
        write2[...] = twice(erase * rate)
        replace2[...] = twice(replace)
        query2[...] = twice(flat(query_ref[...]))
        decay2[...] = twice(flat(decay_ref[...]))
        readout[...] = jnp.zeros_like(readout)

    def wide(ref):
        return jnp.concatenate([ref[...]] * (span // (2 * channel)), axis=-1)

    across = lax.broadcasted_iota(jnp.int32, (span, span), 0) // channel
    down = lax.broadcasted_iota(jnp.int32, (span, span), 1) // channel
    block_ones = (across == down).astype(f32).astype(bf16)
    value = value_ref[...].reshape(rows, channel)
    for part in range(width // span):
        lanes = slice(part * span, (part + 1) * span)
        first = (step * width + part * span) // channel
        spread = (
            (
                lax.broadcasted_iota(jnp.int32, (channel, span), 0)
                == lax.broadcasted_iota(jnp.int32, (channel, span), 1) // channel + first
            )
            .astype(f32)
            .astype(bf16)
        )
        collect = (
            (
                lax.broadcasted_iota(jnp.int32, (span, channel), 0) // channel + first
                == lax.broadcasted_iota(jnp.int32, (span, channel), 1)
            )
            .astype(f32)
            .astype(bf16)
        )
        memory = state_ref[:, :, lanes].reshape(rows, span)
        removed = split_dot(memory * wide(erase2), block_ones)
        value_wide = jnp.dot(value, spread, preferred_element_type=f32)
        memory = (
            memory * wide(decay2) - removed * wide(write2) + value_wide * wide(replace2)
        )
        new_ref[:, :, lanes] = memory.reshape(seqs, heads, span)
        readout[...] += split_dot(memory * wide(query2), collect)

    @pl.when(step == pl.num_programs(0) - 1)
    def _():
        result = readout[...]
        centered = result - jnp.mean(result, axis=-1, keepdims=True)
        variance = jnp.mean(centered * centered, axis=-1, keepdims=True)
        gain = jnp.broadcast_to(attend_ref[...][None], (seqs, heads, channel)).reshape(
            rows, channel
        )
        extra = jnp.broadcast_to(extra_ref[...][None], (seqs, heads, channel)).reshape(
            rows, channel
        )
        bonus = jnp.sum(
            query2[:, :channel] * replace2[:, :channel] * extra, axis=-1, keepdims=True
        )
        mixed = centered * lax.rsqrt(variance + group_eps) * gain + bonus * value.astype(f32)
        mixed_ref[...] = mixed.astype(bf16).reshape(seqs, heads, channel)


def output_kernel(where_ref, mixed_ref, own_ref, near_ref, far_ref, out_ref):
    place, core = where_ref[1], where_ref[2]
    depth, columns = own_ref.shape
    half = depth // 2
    mixed = mixed_ref[:, :depth]
    near = mixed_ref[:, pl.ds(pl.multiple_of(core * half, half), half)]
    far = mixed_ref[:, pl.ds(pl.multiple_of((1 - core) * half, half), half)]
    for kp in range(near_ref.shape[0] + 1):
        if kp == 0:
            result = jnp.dot(mixed, own_ref[...], preferred_element_type=f32)
        else:
            result = jnp.dot(near, near_ref[kp - 1], preferred_element_type=f32) + jnp.dot(
                far, far_ref[kp - 1], preferred_element_type=f32
            )
        at = pl.multiple_of((place ^ kp) * columns, columns)
        out_ref[:, pl.ds(at, columns)] = result.astype(bf16)


def residual_kernel(
    where_ref, *refs
):
    parts, (rows_ref, tail_ref, gain_ref, pick_ref, chosen_ref, own_ref, held) = (
        refs[:GROUPS],
        refs[GROUPS:],
    )
    plane = where_ref[0]
    seqs = rows_ref.shape[0] // GROUPS
    width = rows_ref.shape[1]
    columns = width // GROUPS
    for k, part_ref in enumerate(parts):
        at = pl.multiple_of((plane ^ k) * columns, columns)
        for j in range(GROUPS):
            mine = slice((k ^ j) * seqs, ((k ^ j) + 1) * seqs)
            held[mine, pl.ds(at, columns)] = rows_ref[mine, pl.ds(at, columns)].astype(
                f32
            ) + part_ref[j * seqs : (j + 1) * seqs, :].astype(f32)
    residual = held[...].astype(bf16)
    own_ref[...] = residual[:seqs]
    second = rms_rows(residual.astype(f32), gain_ref[...])
    pick = pick_ref[...]
    chosen_ref[:, :width] = jnp.dot(pick, second, preferred_element_type=f32).astype(bf16)
    chosen_ref[:, width:] = jnp.dot(pick, tail_ref[...], preferred_element_type=f32).astype(bf16)


def expert_kernel(
    members, where_ref, own_ref, other_ref, switch_ref, widen_ref, shrink_ref, mine_ref, theirs_ref, total
):
    step = pl.program_id(0)
    width = switch_ref.shape[0]
    count = own_ref.shape[0]

    @pl.when(step == 0)
    def _():
        total[...] = jnp.zeros_like(total)

    rows = jnp.concatenate([own_ref[:, :width], other_ref[:, :width]], axis=0)
    gate = jnp.dot(rows, switch_ref[...], preferred_element_type=f32)
    up = jnp.dot(rows, widen_ref[...], preferred_element_type=f32)
    hidden = (gate * jax.nn.sigmoid(gate) * up).astype(bf16)
    total[...] += jnp.dot(hidden, shrink_ref[...], preferred_element_type=f32)

    @pl.when(step == pl.num_programs(0) - 1)
    def _():
        member = where_ref[3]
        for ref, out_ref, start in ((own_ref, mine_ref, 0), (other_ref, theirs_ref, count)):
            tail = ref[:, width:].astype(f32)
            lane = lax.broadcasted_iota(jnp.int32, tail.shape, 1)
            share = jnp.sum(
                jnp.where((lane == member) | (lane == member + members), tail, 0.0),
                axis=-1,
                keepdims=True,
            )
            out_ref[...] = (total[start : start + count, :] * share).astype(bf16)


def swap(rows, mask):
    count = lax.axis_size("ep")
    return lax.ppermute(rows, "ep", [(i, i ^ mask) for i in range(count)])


def layered(
    latest_embeddings,
    prior_memory_grids,
    earlier_rescale_gain,
    query_map,
    lookup_map,
    content_map,
    forget_lower_map,
    forget_upper_map,
    forget_shift,
    adapt_lower_map,
    adapt_upper_map,
    adapt_shift,
    erase_lookup_gains,
    substitute_lookup_gains,
    present_extra_gains,
    attender_rescale_gain,
    result_map,
    later_rescale_gain,
    specialist_switch_maps,
    specialist_widen_maps,
    specialist_shrink_maps,
    picked_specialists,
    specialist_picked_shares,
):
    seqs, width = latest_embeddings.shape
    heads = prior_memory_grids.shape[1]
    channel = width // heads
    devices = lax.axis_size("ep")
    members = devices // GROUPS
    chips = members // 2
    columns = query_map.shape[1]
    me = lax.axis_index("ep").astype(jnp.int32)
    core, place, plane = me % 2, (me // 2) % chips, me // members
    where = jnp.stack([plane, place, core, me % members])
    smem = pl.BlockSpec(memory_space=pltpu.SMEM)
    vmem = pl.BlockSpec(memory_space=pltpu.VMEM)
    same_core = [[2 * i + c for i in range(devices // 2)] for c in range(2)]
    same_plane = [
        [members * z + 2 * i + c for i in range(chips)] for z in range(GROUPS) for c in range(2)
    ]

    line = [latest_embeddings] + [swap(latest_embeddings, members * k) for k in range(1, GROUPS)]
    line_rows = jnp.concatenate(line, axis=0)
    gathered = [line_rows] + [swap(line_rows, 2 * k) for k in range(1, chips)]

    stacked = jnp.concatenate([query_map, lookup_map, content_map, result_map], axis=1)
    paired = swap(stacked, 1)
    lower = jnp.where(core == 0, stacked, paired)
    upper = jnp.where(core == 0, paired, stacked)
    chip_maps = jnp.stack(
        [lower.reshape(width, 4, columns), upper.reshape(width, 4, columns)], axis=2
    ).reshape(width, 4 * 2 * columns)
    project_maps = chip_maps[:, : 3 * 2 * columns]
    output_map = chip_maps[:, 3 * 2 * columns :]

    normed = rms_rows(latest_embeddings.astype(f32), earlier_rescale_gain)
    decay_low = jnp.tanh(
        jnp.dot(normed, forget_lower_map, preferred_element_type=f32)
    ).astype(bf16)
    decay = jnp.exp(
        -math.exp(-0.5)
        * jax.nn.sigmoid(
            forget_shift + jnp.dot(decay_low, forget_upper_map, preferred_element_type=f32)
        )
    ).reshape(seqs, heads, channel)
    rate_low = jnp.dot(normed, adapt_lower_map, preferred_element_type=f32).astype(bf16)
    rate = jax.nn.sigmoid(
        adapt_shift + jnp.dot(rate_low, adapt_upper_map, preferred_element_type=f32)
    ).reshape(seqs, heads, channel)

    top_count = picked_specialists.shape[1]
    group = picked_specialists[:, 0] // members
    share_at = (
        picked_specialists[:, :, None] % members == jnp.arange(members, dtype=jnp.int32)
    ).astype(f32)
    shares = jnp.sum(share_at * specialist_picked_shares[:, :, None], axis=1)
    share_high = shares.astype(bf16)
    share_low = (shares - share_high.astype(f32)).astype(bf16)
    tail_width = -(-(2 * members + 1) // 128) * 128
    tail = jnp.concatenate(
        [
            share_high,
            share_low,
            group[:, None].astype(bf16),
            jnp.zeros((seqs, tail_width - 2 * members - 1), bf16),
        ],
        axis=1,
    )

    all_rows = seqs * GROUPS * chips
    projected = pl.pallas_call(
        functools.partial(project_kernel, chips),
        out_shape=jax.ShapeDtypeStruct((all_rows, 6 * columns), bf16),
        in_specs=[smem] + [vmem] * (chips + 2),
        out_specs=vmem,
        name="project",
    )(where, *gathered, earlier_rescale_gain.reshape(1, width), project_maps)
    arrived = lax.all_to_all(
        projected, "ep", split_axis=0, concat_axis=0, tiled=True, axis_index_groups=same_core
    )
    signals = (
        arrived.reshape(devices // 2, seqs, 3, heads * 2 // devices, channel)
        .transpose(2, 1, 0, 3, 4)
        .reshape(3, seqs, heads, channel)
    )

    half = lax.dynamic_slice_in_dim(output_map, core * (width // 2), width // 2, axis=0)
    half, projected_done = lax.optimization_barrier((half, projected))
    near = jnp.stack([swap(half, 2 * k) for k in range(1, chips)])
    far = swap(near, 1)

    lanes = 512
    small = pl.BlockSpec((seqs, heads, channel), lambda i: (0, 0, 0))
    gains = pl.BlockSpec((heads, channel), lambda i: (0, 0))
    block = pl.BlockSpec((seqs, heads, lanes), lambda i: (0, 0, i))
    tile = pltpu.VMEM((seqs * heads, 2 * channel), f32)
    new_state, mixed = pl.pallas_call(
        functools.partial(state_kernel, channel),
        grid=(channel * channel // lanes,),
        out_shape=[
            jax.ShapeDtypeStruct(prior_memory_grids.shape, f32),
            jax.ShapeDtypeStruct((seqs, heads, channel), bf16),
        ],
        in_specs=[small] * 5 + [gains] * 4 + [block],
        out_specs=[block, small],
        scratch_shapes=[tile] * 5 + [pltpu.VMEM((seqs * heads, channel), f32)],
        compiler_params=pltpu.CompilerParams(
            dimension_semantics=("arbitrary",), vmem_limit_bytes=48 * 2**20
        ),
        name="state",
    )(
        signals[1],
        signals[0],
        signals[2],
        decay,
        rate,
        erase_lookup_gains.reshape(heads, channel),
        substitute_lookup_gains.reshape(heads, channel),
        present_extra_gains.reshape(heads, channel),
        attender_rescale_gain.reshape(heads, channel),
        prior_memory_grids,
    )

    mixed_rows = jnp.concatenate([mixed.reshape(seqs, width), tail], axis=1)
    mixed_line = jnp.concatenate(
        [mixed_rows] + [swap(mixed_rows, members * k) for k in range(1, GROUPS)], axis=0
    )
    line_columns = pl.pallas_call(
        output_kernel,
        out_shape=jax.ShapeDtypeStruct((GROUPS * seqs, width // GROUPS), bf16),
        in_specs=[smem] + [vmem] * 4,
        out_specs=vmem,
        name="output",
    )(where, mixed_line, output_map, near, far)
    parts = [line_columns] + [swap(line_columns, members * k) for k in range(1, GROUPS)]

    room = (seqs + 1) // 2
    line_tail = mixed_line[:, width:]
    line_group = line_tail[:, 2 * members].reshape(GROUPS, seqs)
    wanted = (line_group == plane.astype(bf16)).astype(jnp.int32)
    rank = jnp.cumsum(wanted, axis=1) - wanted
    pick = (
        (wanted[:, None, :] == 1)
        & (rank[:, None, :] == jnp.arange(room, dtype=jnp.int32)[None, :, None])
    ).astype(bf16)
    pick = (
        pick[:, :, None, :] * jnp.eye(GROUPS, dtype=bf16)[:, None, :, None]
    ).reshape(GROUPS * room, GROUPS * seqs)
    chosen, residual = pl.pallas_call(
        residual_kernel,
        out_shape=[
            jax.ShapeDtypeStruct((GROUPS * room, width + tail_width), bf16),
            jax.ShapeDtypeStruct((seqs, width), bf16),
        ],
        in_specs=[smem] + [vmem] * (GROUPS + 4),
        out_specs=[vmem] * 2,
        scratch_shapes=[pltpu.VMEM((GROUPS * seqs, width), f32)],
        name="residual",
    )(where, *parts, line_rows, line_tail, later_rescale_gain.reshape(1, width), pick)

    own_rows = lax.all_gather(chosen, "ep", axis=0, tiled=True, axis_index_groups=same_plane)
    other_rows = swap(own_rows, 1)
    hidden = specialist_switch_maps.shape[2]
    piece = hidden // 2
    count = own_rows.shape[0]
    mine, theirs = pl.pallas_call(
        functools.partial(expert_kernel, members),
        grid=(hidden // piece,),
        out_shape=[jax.ShapeDtypeStruct((count, width), bf16)] * 2,
        in_specs=[
            smem,
            full(own_rows.shape),
            full(own_rows.shape),
            pl.BlockSpec((None, width, piece), lambda i: (0, 0, i)),
            pl.BlockSpec((None, width, piece), lambda i: (0, 0, i)),
            pl.BlockSpec((None, piece, width), lambda i: (0, i, 0)),
        ],
        out_specs=[full((count, width))] * 2,
        scratch_shapes=[pltpu.VMEM((2 * count, width), f32)],
        compiler_params=pltpu.CompilerParams(
            dimension_semantics=("arbitrary",), vmem_limit_bytes=48 * 2**20
        ),
        name="expert",
    )(
        where,
        own_rows,
        other_rows,
        specialist_switch_maps,
        specialist_widen_maps,
        specialist_shrink_maps,
    )

    both = (mine.astype(f32) + swap(theirs, 1).astype(f32)).astype(bf16)
    spread = lax.all_to_all(
        both, "ep", split_axis=0, concat_axis=0, tiled=True, axis_index_groups=same_plane
    )
    summed = jnp.sum(
        spread.reshape(chips, GROUPS, room, width).astype(f32), axis=0
    ).astype(bf16)
    home = jnp.concatenate(
        [summed[0]] + [swap(summed[k], members * k) for k in range(1, GROUPS)], axis=0
    )
    own_rank = jnp.sum(
        (group[None, :] == group[:, None]) & (jnp.arange(seqs)[None, :] < jnp.arange(seqs)[:, None]),
        axis=1,
    ).astype(jnp.int32)
    slot = (group ^ plane) * room + own_rank
    fetch = (slot[:, None] == jnp.arange(GROUPS * room, dtype=jnp.int32)[None, :]).astype(bf16)
    expert_sum = jnp.dot(fetch, home, preferred_element_type=f32)
    new_hidden = (residual.astype(f32) + expert_sum).astype(bf16)
    return (new_hidden, new_state)


def rms_norm(rows_in, gain):
    values = rows_in.astype(jnp.float32)
    scale = lax.rsqrt(jnp.mean(values * values, axis=-1, keepdims=True) + norm_eps)
    return (values * scale * gain).astype(jnp.bfloat16)


def memory_readout(
    query_signal,
    substitute_lookup,
    content_signals,
    forget_multiplier,
    adapt_speed,
    erase_signal,
    memory_grid,
    attender_rescale_gain,
    present_extra_gains,
):
    highest = lax.Precision.HIGHEST
    removed = jnp.einsum("bhij,bhj->bhi", memory_grid, erase_signal, precision=highest)
    memory_grid = (
        memory_grid * forget_multiplier[:, :, None, :]
        - removed[..., None] * (erase_signal * adapt_speed)[:, :, None, :]
        + content_signals[..., None] * substitute_lookup[:, :, None, :]
    )
    readout = jnp.einsum("bhij,bhj->bhi", memory_grid, query_signal, precision=highest)
    centered = readout - jnp.mean(readout, axis=-1, keepdims=True)
    variance = jnp.mean(centered * centered, axis=-1, keepdims=True)
    rescaled_result = centered * lax.rsqrt(variance + group_eps) * attender_rescale_gain
    present_extra = (
        jnp.sum(query_signal * substitute_lookup * present_extra_gains, axis=-1, keepdims=True)
        * content_signals
    )
    return (rescaled_result + present_extra, memory_grid)


def local(
    latest_embeddings,
    prior_memory_grids,
    earlier_rescale_gain,
    query_map,
    lookup_map,
    content_map,
    forget_lower_map,
    forget_upper_map,
    forget_shift,
    adapt_lower_map,
    adapt_upper_map,
    adapt_shift,
    erase_lookup_gains,
    substitute_lookup_gains,
    present_extra_gains,
    attender_rescale_gain,
    result_map,
    later_rescale_gain,
    specialist_switch_maps,
    specialist_widen_maps,
    specialist_shrink_maps,
    picked_specialists,
    specialist_picked_shares,
):
    seq_count, model_width = latest_embeddings.shape
    attender_count = prior_memory_grids.shape[1]
    channel_span = model_width // attender_count
    devices = lax.axis_size("ep")
    columns = query_map.shape[1]
    normed = rms_norm(latest_embeddings, earlier_rescale_gain)
    stacked = jnp.concatenate([query_map, lookup_map, content_map], axis=1)
    projected = jnp.dot(
        lax.all_gather(normed, "ep", axis=0, tiled=True),
        stacked,
        preferred_element_type=jnp.float32,
    ).astype(jnp.bfloat16)
    query_signal, key_rows, content_signals = (
        lax.all_to_all(projected[:, :columns], "ep", split_axis=0, concat_axis=1, tiled=True),
        lax.all_to_all(
            projected[:, columns : 2 * columns], "ep", split_axis=0, concat_axis=1, tiled=True
        ),
        lax.all_to_all(projected[:, 2 * columns :], "ep", split_axis=0, concat_axis=1, tiled=True),
    )
    decay_low = jnp.tanh(
        jnp.dot(normed, forget_lower_map, preferred_element_type=jnp.float32)
    ).astype(jnp.bfloat16)
    forget_multiplier = jnp.exp(
        -math.exp(-0.5)
        * jax.nn.sigmoid(
            forget_shift + jnp.dot(decay_low, forget_upper_map, preferred_element_type=jnp.float32)
        )
    )
    rate_low = jnp.dot(normed, adapt_lower_map, preferred_element_type=jnp.float32).astype(
        jnp.bfloat16
    )
    adapt_speed = jax.nn.sigmoid(
        adapt_shift + jnp.dot(rate_low, adapt_upper_map, preferred_element_type=jnp.float32)
    )
    key_float = key_rows.astype(jnp.float32)
    erase_signal = (key_float * erase_lookup_gains).reshape(seq_count, attender_count, channel_span)
    erase_signal = erase_signal * lax.rsqrt(
        jnp.sum(erase_signal * erase_signal, axis=-1, keepdims=True) + unit_eps
    )
    substitute_lookup = key_float * (1.0 + (adapt_speed - 1.0) * substitute_lookup_gains)
    head_shape = (seq_count, attender_count, channel_span)
    mixed_heads, memory_grid = memory_readout(
        query_signal.astype(jnp.float32).reshape(head_shape),
        substitute_lookup.reshape(head_shape),
        content_signals.astype(jnp.float32).reshape(head_shape),
        forget_multiplier.reshape(head_shape),
        adapt_speed.reshape(head_shape),
        erase_signal,
        prior_memory_grids.reshape(seq_count, attender_count, channel_span, channel_span),
        attender_rescale_gain.reshape(attender_count, channel_span),
        present_extra_gains.reshape(attender_count, channel_span),
    )
    mixed = mixed_heads.reshape(seq_count, model_width).astype(jnp.bfloat16)
    new_state = memory_grid.reshape(seq_count, attender_count, channel_span * channel_span)
    partial_rows = jnp.dot(
        lax.all_gather(mixed, "ep", axis=0, tiled=True),
        result_map,
        preferred_element_type=jnp.float32,
    ).astype(jnp.bfloat16)
    mixer_out = lax.all_to_all(partial_rows, "ep", split_axis=0, concat_axis=1, tiled=True)
    residual = (latest_embeddings.astype(jnp.float32) + mixer_out.astype(jnp.float32)).astype(
        jnp.bfloat16
    )
    second = rms_norm(residual, later_rescale_gain)
    top_count = picked_specialists.shape[1]
    expert_count = specialist_switch_maps.shape[0] * devices
    group_size = expert_count // GROUPS
    capacity = ((seq_count + 1) // 2 * top_count + group_size - 1) // group_size
    flat_ids = picked_specialists.reshape(-1)
    matches = (flat_ids[:, None] == jnp.arange(expert_count, dtype=jnp.int32)[None, :]).astype(
        jnp.int32
    )
    slot_rank = jnp.sum((jnp.cumsum(matches, axis=0) - matches) * matches, axis=1)
    slot_ids = flat_ids * capacity + slot_rank
    picks = (
        slot_ids[:, None] == jnp.arange(expert_count * capacity, dtype=jnp.int32)[None, :]
    ).astype(jnp.bfloat16)
    repeated = jnp.repeat(second, top_count, axis=0)
    send_rows = jnp.einsum("sk,sd->kd", picks, repeated, preferred_element_type=jnp.float32).astype(
        jnp.bfloat16
    )
    send_rows = send_rows.reshape(devices, expert_count // devices * capacity, model_width)
    received = lax.all_to_all(send_rows, "ep", split_axis=0, concat_axis=0, tiled=True)
    rows_in = received.reshape(-1, model_width)
    gate_proj = jnp.dot(rows_in, specialist_switch_maps[0], preferred_element_type=jnp.float32)
    up_proj = jnp.dot(rows_in, specialist_widen_maps[0], preferred_element_type=jnp.float32)
    hidden_act = (jax.nn.silu(gate_proj) * up_proj).astype(jnp.bfloat16)
    results = jnp.dot(
        hidden_act, specialist_shrink_maps[0], preferred_element_type=jnp.float32
    ).astype(jnp.bfloat16)
    returned = lax.all_to_all(
        results.reshape(received.shape), "ep", split_axis=0, concat_axis=0, tiled=True
    )
    collected = jnp.dot(
        picks, returned.reshape(-1, model_width), preferred_element_type=jnp.float32
    )
    expert_sum = jnp.sum(
        collected.reshape(seq_count, top_count, model_width) * specialist_picked_shares[:, :, None],
        axis=1,
    )
    new_hidden = (residual.astype(jnp.float32) + expert_sum).astype(jnp.bfloat16)
    return (new_hidden, new_state)


def step(*args):
    devices, columns = lax.axis_size("ep"), args[3].shape[1]
    if devices % (2 * GROUPS) == 0 and (2 * columns) % 128 == 0 and args[18].shape[0] == 1:
        return layered(*args)
    return local(*args)


def solution(mesh):
    return jax.shard_map(
        step,
        mesh=mesh,
        in_specs=(
            P("ep", None),
            P("ep", None, None),
            P(),
            P(None, "ep"),
            P(None, "ep"),
            P(None, "ep"),
            P(),
            P(),
            P(),
            P(),
            P(),
            P(),
            P(),
            P(),
            P(),
            P(),
            P(None, "ep"),
            P(),
            P("ep", None, None),
            P("ep", None, None),
            P("ep", None, None),
            P("ep", None),
            P("ep", None),
        ),
        out_specs=(P("ep", None), P("ep", None, None)),
        check_vma=False,
    )
```

```python
import functools
import math

import jax
import jax.numpy as jnp
from jax import lax
from jax.experimental import pallas as pl
from jax.experimental.pallas import tpu as pltpu
from jax.sharding import PartitionSpec as P

GROUPS = 4


norm_eps = 1e-06
group_eps = 0.00064
unit_eps = 1e-06

f32 = jnp.float32
bf16 = jnp.bfloat16


def full(shape):
    return pl.BlockSpec(shape, lambda *_: (0,) * len(shape))


def rms_rows(values, gain):
    scale = lax.rsqrt(jnp.mean(values * values, axis=-1, keepdims=True) + norm_eps)
    return (values * scale * gain).astype(bf16)


def split_dot(values, selector):
    high = values.astype(bf16)
    low = (values - high.astype(f32)).astype(bf16)
    return jnp.dot(high, selector, preferred_element_type=f32) + jnp.dot(
        low, selector, preferred_element_type=f32
    )


def turned_dot(rows, columns):
    return lax.dot_general(rows, columns, (((1,), (1,)), ((), ())), preferred_element_type=f32)


def project_kernel(chips, where_ref, *refs):
    rows_refs, (gain_ref, *map_refs, out_ref, maps) = refs[:chips], refs[chips:]
    plane, place, core = where_ref[0], where_ref[1], where_ref[2]
    own_refs, pair_refs = map_refs[:3], map_refs[3:]
    columns = own_refs[0].shape[0]

    def lay(lower_refs, upper_refs):
        for m in range(3):
            maps[2 * m * columns : (2 * m + 1) * columns, :] = lower_refs[m][...]
            maps[(2 * m + 1) * columns : (2 * m + 2) * columns, :] = upper_refs[m][...]

    pl.when(core == 0)(lambda: lay(own_refs, pair_refs))
    pl.when(core != 0)(lambda: lay(pair_refs, own_refs))
    normed = jnp.concatenate(
        [rms_rows(ref[...].astype(f32), gain_ref[...]) for ref in rows_refs], axis=0
    )
    result = turned_dot(normed, maps[...]).astype(bf16)
    seqs = result.shape[0] // (GROUPS * chips)
    for kp in range(chips):
        for kz in range(GROUPS):
            chip = (plane ^ kz) * chips + (place ^ kp)
            block = (kp * GROUPS + kz) * seqs
            out_ref[pl.ds(pl.multiple_of(chip * seqs, seqs), seqs), :] = result[
                block : block + seqs
            ]


def state_kernel(
    channel,
    key_ref,
    query_ref,
    value_ref,
    decay_ref,
    rate_ref,
    erase_ref,
    substitute_ref,
    extra_ref,
    attend_ref,
    state_ref,
    new_ref,
    mixed_ref,
    erase2,
    write2,
    replace2,
    query2,
    decay2,
    readout,
):
    step = pl.program_id(0)
    seqs, heads, width = state_ref.shape
    rows = seqs * heads
    span = 256

    def flat(x):
        return x.astype(f32).reshape(rows, channel)

    def twice(x):
        return jnp.concatenate([x, x], axis=-1)

    @pl.when(step == 0)
    def _():
        key = flat(key_ref[...])
        rate = flat(rate_ref[...])
        erase = (key.reshape(seqs, heads, channel) * erase_ref[...][None]).reshape(rows, channel)
        erase = erase * lax.rsqrt(jnp.sum(erase * erase, axis=-1, keepdims=True) + unit_eps)
        gain = jnp.broadcast_to(substitute_ref[...][None], (seqs, heads, channel)).reshape(
            rows, channel
        )
        replace = key * (1.0 + (rate - 1.0) * gain)
        erase2[...] = twice(erase)
        write2[...] = twice(erase * rate)
        replace2[...] = twice(replace)
        query2[...] = twice(flat(query_ref[...]))
        decay2[...] = twice(flat(decay_ref[...]))
        readout[...] = jnp.zeros_like(readout)

    def wide(ref):
        return jnp.concatenate([ref[...]] * (span // (2 * channel)), axis=-1)

    across = lax.broadcasted_iota(jnp.int32, (span, span), 0) // channel
    down = lax.broadcasted_iota(jnp.int32, (span, span), 1) // channel
    block_ones = (across == down).astype(f32).astype(bf16)
    value = value_ref[...].reshape(rows, channel)
    for part in range(width // span):
        lanes = slice(part * span, (part + 1) * span)
        first = (step * width + part * span) // channel
        spread = (
            (
                lax.broadcasted_iota(jnp.int32, (channel, span), 0)
                == lax.broadcasted_iota(jnp.int32, (channel, span), 1) // channel + first
            )
            .astype(f32)
            .astype(bf16)
        )
        collect = (
            (
                lax.broadcasted_iota(jnp.int32, (span, channel), 0) // channel + first
                == lax.broadcasted_iota(jnp.int32, (span, channel), 1)
            )
            .astype(f32)
            .astype(bf16)
        )
        memory = state_ref[:, :, lanes].reshape(rows, span)
        removed = jnp.dot(
            (memory * wide(erase2)).astype(bf16), block_ones, preferred_element_type=f32
        )
        value_wide = jnp.dot(value, spread, preferred_element_type=f32)
        memory = (
            memory * wide(decay2) - removed * wide(write2) + value_wide * wide(replace2)
        )
        new_ref[:, :, lanes] = memory.reshape(seqs, heads, span)
        readout[...] += split_dot(memory * wide(query2), collect)

    @pl.when(step == pl.num_programs(0) - 1)
    def _():
        result = readout[...]
        centered = result - jnp.mean(result, axis=-1, keepdims=True)
        variance = jnp.mean(centered * centered, axis=-1, keepdims=True)
        gain = jnp.broadcast_to(attend_ref[...][None], (seqs, heads, channel)).reshape(
            rows, channel
        )
        extra = jnp.broadcast_to(extra_ref[...][None], (seqs, heads, channel)).reshape(
            rows, channel
        )
        bonus = jnp.sum(
            query2[:, :channel] * replace2[:, :channel] * extra, axis=-1, keepdims=True
        )
        mixed = centered * lax.rsqrt(variance + group_eps) * gain + bonus * value.astype(f32)
        mixed_ref[...] = mixed.astype(bf16).reshape(seqs, heads, channel)


def output_kernel(room, members, where_ref, *refs):
    mixed_refs, (own_ref, near_ref, far_ref) = refs[:GROUPS], refs[GROUPS : GROUPS + 3]
    part_refs, (pick_ref, tail_ref, mixed, result) = refs[GROUPS + 3 : 2 * GROUPS + 3], refs[2 * GROUPS + 3 :]
    plane, place, core = where_ref[0], where_ref[1], where_ref[2]
    columns, depth = own_ref.shape
    half = depth // 2
    seqs = mixed_refs[0].shape[0]
    rows = GROUPS * seqs
    for k, ref in enumerate(mixed_refs):
        mixed[k * seqs : (k + 1) * seqs, :] = ref[...]
    near = mixed[:, pl.ds(pl.multiple_of(core * half, half), half)]
    far = mixed[:, pl.ds(pl.multiple_of((1 - core) * half, half), half)]
    for kp in range(near_ref.shape[0] + 1):
        if kp == 0:
            block = turned_dot(mixed[:, :depth], own_ref[...])
        else:
            block = turned_dot(near, near_ref[kp - 1]) + turned_dot(far, far_ref[kp - 1])
        at = pl.multiple_of((place ^ kp) * columns, columns)
        result[:, pl.ds(at, columns)] = block.astype(bf16)

    def iota(shape, axis):
        return lax.broadcasted_iota(jnp.int32, shape, axis)

    tail = mixed[:, depth:]
    at = iota(tail.shape, 1) == 2 * members
    group = jnp.sum(jnp.where(at, tail.astype(f32), 0.0), axis=1, keepdims=True)
    above, along = iota((rows, rows), 0), iota((rows, rows), 1)
    group_row = jnp.sum(jnp.where(above == along, group, 0.0), axis=0, keepdims=True)
    earlier = (above // seqs == along // seqs) & (above < along) & (group == group_row)
    rank = jnp.sum(earlier.astype(f32), axis=0, keepdims=True)
    slot, lane = iota((GROUPS * room, rows), 0), iota((GROUPS * room, rows), 1)
    for k, part_ref in enumerate(part_refs):
        pick = (
            (lane // seqs == ((slot // room) ^ k))
            & (group_row == (plane ^ k).astype(f32))
            & (rank == (slot % room).astype(f32))
        )
        pick = pick.astype(f32).astype(bf16)
        part_ref[...] = jnp.dot(pick, result[...], preferred_element_type=f32).astype(bf16)
        if k == 0:
            pick_ref[...] = pick
            tail_ref[...] = jnp.dot(pick, tail, preferred_element_type=f32).astype(bf16)


def residual_kernel(where_ref, *refs):
    parts, (rows_ref, tail_ref, gain_ref, chosen_ref, residual_ref, held) = (
        refs[:GROUPS],
        refs[GROUPS:],
    )
    plane = where_ref[0]
    width = rows_ref.shape[1]
    columns = width // GROUPS
    for k, part_ref in enumerate(parts):
        at = pl.multiple_of((plane ^ k) * columns, columns)
        held[:, pl.ds(at, columns)] = rows_ref[:, pl.ds(at, columns)].astype(f32) + part_ref[
            ...
        ].astype(f32)
    residual = held[...].astype(bf16)
    residual_ref[...] = residual
    chosen_ref[:, :width] = rms_rows(residual.astype(f32), gain_ref[...])
    chosen_ref[:, width:] = tail_ref[...]


def expert_kernel(members, where_ref, *refs):
    blocks, (switch_ref, widen_ref, shrink_ref, mine_ref, theirs_ref, rows) = (
        refs[:members],
        refs[members:],
    )
    width = switch_ref.shape[1]
    size = blocks[0].shape[0]
    for i, ref in enumerate(blocks):
        rows[i * size : (i + 1) * size, :] = ref[...]
    tokens = rows[:, :width]
    gate = jnp.dot(tokens, switch_ref[0], preferred_element_type=f32)
    up = jnp.dot(tokens, widen_ref[0], preferred_element_type=f32)
    hidden = (gate * jax.nn.sigmoid(gate) * up).astype(bf16)
    tail = rows[:, width:].astype(f32)
    lane = lax.broadcasted_iota(jnp.int32, tail.shape, 1)
    member = where_ref[3]
    share = jnp.sum(
        jnp.where((lane == member) | (lane == member + members), tail, 0.0), axis=-1, keepdims=True
    )
    result = jnp.dot(hidden, shrink_ref[0], preferred_element_type=f32) * share
    half = result.shape[0] // 2
    mine_ref[...] = result[:half].astype(bf16)
    theirs_ref[...] = result[half:].astype(bf16)


def swap(rows, mask):
    count = lax.axis_size("ep")
    return lax.ppermute(rows, "ep", [(i, i ^ mask) for i in range(count)])


def layered(
    latest_embeddings,
    prior_memory_grids,
    earlier_rescale_gain,
    query_map,
    lookup_map,
    content_map,
    forget_lower_map,
    forget_upper_map,
    forget_shift,
    adapt_lower_map,
    adapt_upper_map,
    adapt_shift,
    erase_lookup_gains,
    substitute_lookup_gains,
    present_extra_gains,
    attender_rescale_gain,
    result_map,
    later_rescale_gain,
    specialist_switch_maps,
    specialist_widen_maps,
    specialist_shrink_maps,
    picked_specialists,
    specialist_picked_shares,
):
    seqs, width = latest_embeddings.shape
    heads = prior_memory_grids.shape[1]
    channel = width // heads
    devices = lax.axis_size("ep")
    members = devices // GROUPS
    chips = members // 2
    columns = query_map.shape[1]
    me = lax.axis_index("ep").astype(jnp.int32)
    core, place, plane = me % 2, (me // 2) % chips, me // members
    where = jnp.stack([plane, place, core, me % members])
    smem = pl.BlockSpec(memory_space=pltpu.SMEM)
    vmem = pl.BlockSpec(memory_space=pltpu.VMEM)
    same_core = [[2 * i + c for i in range(devices // 2)] for c in range(2)]

    def limit(mib):
        return pltpu.CompilerParams(vmem_limit_bytes=mib * 2**20)

    line = [latest_embeddings] + [swap(latest_embeddings, members * k) for k in range(1, GROUPS)]
    line_rows = jnp.concatenate(line, axis=0)
    gathered = [line_rows] + [swap(line_rows, 2 * k) for k in range(1, chips)]

    own_maps = [m.T for m in (query_map, lookup_map, content_map, result_map)]
    pair_maps = [swap(m, 1) for m in own_maps]

    normed = rms_rows(line_rows[:seqs].astype(f32), earlier_rescale_gain)
    decay_low = jnp.tanh(
        jnp.dot(normed, forget_lower_map, preferred_element_type=f32)
    ).astype(bf16)
    decay = jnp.exp(
        -math.exp(-0.5)
        * jax.nn.sigmoid(
            forget_shift + jnp.dot(decay_low, forget_upper_map, preferred_element_type=f32)
        )
    ).reshape(seqs, heads, channel)
    rate_low = jnp.dot(normed, adapt_lower_map, preferred_element_type=f32).astype(bf16)
    rate = jax.nn.sigmoid(
        adapt_shift + jnp.dot(rate_low, adapt_upper_map, preferred_element_type=f32)
    ).reshape(seqs, heads, channel)

    top_count = picked_specialists.shape[1]
    group = picked_specialists[:, 0] // members
    share_at = (
        picked_specialists[:, :, None] % members == jnp.arange(members, dtype=jnp.int32)
    ).astype(f32)
    shares = jnp.sum(share_at * specialist_picked_shares[:, :, None], axis=1)
    share_high = shares.astype(bf16)
    share_low = (shares - share_high.astype(f32)).astype(bf16)
    tail_width = -(-(2 * members + 1) // 128) * 128
    tail = jnp.concatenate(
        [
            share_high,
            share_low,
            group[:, None].astype(bf16),
            jnp.zeros((seqs, tail_width - 2 * members - 1), bf16),
        ],
        axis=1,
    )

    all_rows = seqs * GROUPS * chips
    projected = pl.pallas_call(
        functools.partial(project_kernel, chips),
        out_shape=jax.ShapeDtypeStruct((all_rows, 6 * columns), bf16),
        in_specs=[smem] + [vmem] * (chips + 7),
        out_specs=vmem,
        scratch_shapes=[pltpu.VMEM((6 * columns, width), bf16)],
        compiler_params=limit(16),
        name="project",
    )(where, *gathered, earlier_rescale_gain.reshape(1, width), *own_maps[:3], *pair_maps[:3])
    arrived = lax.all_to_all(
        projected, "ep", split_axis=0, concat_axis=0, tiled=True, axis_index_groups=same_core
    )
    signals = (
        arrived.reshape(devices // 2, seqs, 3, heads * 2 // devices, channel)
        .transpose(2, 1, 0, 3, 4)
        .reshape(3, seqs, heads, channel)
    )

    chip_map = jnp.where(
        core == 0,
        jnp.concatenate([own_maps[3], pair_maps[3]], axis=0),
        jnp.concatenate([pair_maps[3], own_maps[3]], axis=0),
    )
    half = lax.dynamic_slice_in_dim(chip_map, core * (width // 2), width // 2, axis=1)
    half, _ = lax.optimization_barrier((half, projected))
    near = jnp.stack([swap(half, 2 * k) for k in range(1, chips)])
    far = swap(near, 1)

    lanes = 1024
    small = pl.BlockSpec((seqs, heads, channel), lambda i: (0, 0, 0))
    gains = pl.BlockSpec((heads, channel), lambda i: (0, 0))
    block = pl.BlockSpec((seqs, heads, lanes), lambda i: (0, 0, i))
    tile = pltpu.VMEM((seqs * heads, 2 * channel), f32)
    new_state, mixed = pl.pallas_call(
        functools.partial(state_kernel, channel),
        grid=(channel * channel // lanes,),
        out_shape=[
            jax.ShapeDtypeStruct(prior_memory_grids.shape, f32),
            jax.ShapeDtypeStruct((seqs, heads, channel), bf16),
        ],
        in_specs=[small] * 5 + [gains] * 4 + [block],
        out_specs=[block, small],
        scratch_shapes=[tile] * 5 + [pltpu.VMEM((seqs * heads, channel), f32)],
        compiler_params=limit(32),
        name="state",
    )(
        signals[1],
        signals[0],
        signals[2],
        decay,
        rate,
        erase_lookup_gains.reshape(heads, channel),
        substitute_lookup_gains.reshape(heads, channel),
        present_extra_gains.reshape(heads, channel),
        attender_rescale_gain.reshape(heads, channel),
        prior_memory_grids,
    )

    mixed_rows = jnp.concatenate([mixed.reshape(seqs, width), tail], axis=1)
    mixed_line = [mixed_rows] + [swap(mixed_rows, members * k) for k in range(1, GROUPS)]
    room = (seqs + 1) // 2
    count = GROUPS * room
    *parts, pick, chosen_tail = pl.pallas_call(
        functools.partial(output_kernel, room, members),
        out_shape=[jax.ShapeDtypeStruct((count, width // GROUPS), bf16)] * GROUPS
        + [
            jax.ShapeDtypeStruct((count, GROUPS * seqs), bf16),
            jax.ShapeDtypeStruct((count, tail_width), bf16),
        ],
        in_specs=[smem] + [vmem] * (GROUPS + 3),
        out_specs=[vmem] * (GROUPS + 2),
        scratch_shapes=[
            pltpu.VMEM((GROUPS * seqs, width + tail_width), bf16),
            pltpu.VMEM((GROUPS * seqs, width // GROUPS), bf16),
        ],
        compiler_params=limit(16),
        name="output",
    )(where, *mixed_line, chip_map, near, far)
    parts = [parts[0]] + [swap(parts[k], members * k) for k in range(1, GROUPS)]
    chosen_rows = jnp.dot(pick, line_rows, preferred_element_type=f32).astype(bf16)
    chosen, residual = pl.pallas_call(
        residual_kernel,
        out_shape=[
            jax.ShapeDtypeStruct((count, width + tail_width), bf16),
            jax.ShapeDtypeStruct((count, width), bf16),
        ],
        in_specs=[smem] + [vmem] * (GROUPS + 3),
        out_specs=[vmem] * 2,
        scratch_shapes=[pltpu.VMEM((count, width), f32)],
        compiler_params=limit(8),
        name="residual",
    )(where, *parts, chosen_rows, chosen_tail, later_rescale_gain.reshape(1, width))

    own_rows = [chosen] + [swap(chosen, 2 * k) for k in range(1, chips)]
    other_rows = [swap(rows, 1) for rows in own_rows]
    mine, theirs = pl.pallas_call(
        functools.partial(expert_kernel, members),
        out_shape=[jax.ShapeDtypeStruct((chips * count, width), bf16)] * 2,
        in_specs=[smem] + [vmem] * (members + 3),
        out_specs=[vmem] * 2,
        scratch_shapes=[pltpu.VMEM((members * count, width + tail_width), bf16)],
        compiler_params=limit(24),
        name="expert",
    )(
        where,
        *own_rows,
        *other_rows,
        specialist_switch_maps,
        specialist_widen_maps,
        specialist_shrink_maps,
    )

    both = (mine.astype(f32) + swap(theirs, 1).astype(f32)).astype(bf16)
    pieces = [both[k * count : (k + 1) * count] for k in range(chips)]
    pieces = [pieces[0]] + [swap(pieces[k], 2 * k) for k in range(1, chips)]
    finished = residual.astype(f32)
    for piece in pieces:
        finished = finished + piece.astype(f32)
    finished = finished.astype(bf16).reshape(GROUPS, room, width)
    home = jnp.concatenate(
        [finished[0]] + [swap(finished[k], members * k) for k in range(1, GROUPS)], axis=0
    )
    earlier = (group[None, :] == group[:, None]) & (
        jnp.arange(seqs)[None, :] < jnp.arange(seqs)[:, None]
    )
    slot = (group ^ plane) * room + jnp.sum(earlier, axis=1).astype(jnp.int32)
    fetch = (slot[:, None] == jnp.arange(count, dtype=jnp.int32)[None, :]).astype(bf16)
    new_hidden = jnp.dot(fetch, home, preferred_element_type=f32).astype(bf16)
    return (new_hidden, new_state)


def rms_norm(rows_in, gain):
    values = rows_in.astype(jnp.float32)
    scale = lax.rsqrt(jnp.mean(values * values, axis=-1, keepdims=True) + norm_eps)
    return (values * scale * gain).astype(jnp.bfloat16)


def memory_readout(
    query_signal,
    substitute_lookup,
    content_signals,
    forget_multiplier,
    adapt_speed,
    erase_signal,
    memory_grid,
    attender_rescale_gain,
    present_extra_gains,
):
    highest = lax.Precision.HIGHEST
    removed = jnp.einsum("bhij,bhj->bhi", memory_grid, erase_signal, precision=highest)
    memory_grid = (
        memory_grid * forget_multiplier[:, :, None, :]
        - removed[..., None] * (erase_signal * adapt_speed)[:, :, None, :]
        + content_signals[..., None] * substitute_lookup[:, :, None, :]
    )
    readout = jnp.einsum("bhij,bhj->bhi", memory_grid, query_signal, precision=highest)
    centered = readout - jnp.mean(readout, axis=-1, keepdims=True)
    variance = jnp.mean(centered * centered, axis=-1, keepdims=True)
    rescaled_result = centered * lax.rsqrt(variance + group_eps) * attender_rescale_gain
    present_extra = (
        jnp.sum(query_signal * substitute_lookup * present_extra_gains, axis=-1, keepdims=True)
        * content_signals
    )
    return (rescaled_result + present_extra, memory_grid)


def local(
    latest_embeddings,
    prior_memory_grids,
    earlier_rescale_gain,
    query_map,
    lookup_map,
    content_map,
    forget_lower_map,
    forget_upper_map,
    forget_shift,
    adapt_lower_map,
    adapt_upper_map,
    adapt_shift,
    erase_lookup_gains,
    substitute_lookup_gains,
    present_extra_gains,
    attender_rescale_gain,
    result_map,
    later_rescale_gain,
    specialist_switch_maps,
    specialist_widen_maps,
    specialist_shrink_maps,
    picked_specialists,
    specialist_picked_shares,
):
    seq_count, model_width = latest_embeddings.shape
    attender_count = prior_memory_grids.shape[1]
    channel_span = model_width // attender_count
    devices = lax.axis_size("ep")
    columns = query_map.shape[1]
    normed = rms_norm(latest_embeddings, earlier_rescale_gain)
    stacked = jnp.concatenate([query_map, lookup_map, content_map], axis=1)
    projected = jnp.dot(
        lax.all_gather(normed, "ep", axis=0, tiled=True),
        stacked,
        preferred_element_type=jnp.float32,
    ).astype(jnp.bfloat16)
    query_signal, key_rows, content_signals = (
        lax.all_to_all(projected[:, :columns], "ep", split_axis=0, concat_axis=1, tiled=True),
        lax.all_to_all(
            projected[:, columns : 2 * columns], "ep", split_axis=0, concat_axis=1, tiled=True
        ),
        lax.all_to_all(projected[:, 2 * columns :], "ep", split_axis=0, concat_axis=1, tiled=True),
    )
    decay_low = jnp.tanh(
        jnp.dot(normed, forget_lower_map, preferred_element_type=jnp.float32)
    ).astype(jnp.bfloat16)
    forget_multiplier = jnp.exp(
        -math.exp(-0.5)
        * jax.nn.sigmoid(
            forget_shift + jnp.dot(decay_low, forget_upper_map, preferred_element_type=jnp.float32)
        )
    )
    rate_low = jnp.dot(normed, adapt_lower_map, preferred_element_type=jnp.float32).astype(
        jnp.bfloat16
    )
    adapt_speed = jax.nn.sigmoid(
        adapt_shift + jnp.dot(rate_low, adapt_upper_map, preferred_element_type=jnp.float32)
    )
    key_float = key_rows.astype(jnp.float32)
    erase_signal = (key_float * erase_lookup_gains).reshape(seq_count, attender_count, channel_span)
    erase_signal = erase_signal * lax.rsqrt(
        jnp.sum(erase_signal * erase_signal, axis=-1, keepdims=True) + unit_eps
    )
    substitute_lookup = key_float * (1.0 + (adapt_speed - 1.0) * substitute_lookup_gains)
    head_shape = (seq_count, attender_count, channel_span)
    mixed_heads, memory_grid = memory_readout(
        query_signal.astype(jnp.float32).reshape(head_shape),
        substitute_lookup.reshape(head_shape),
        content_signals.astype(jnp.float32).reshape(head_shape),
        forget_multiplier.reshape(head_shape),
        adapt_speed.reshape(head_shape),
        erase_signal,
        prior_memory_grids.reshape(seq_count, attender_count, channel_span, channel_span),
        attender_rescale_gain.reshape(attender_count, channel_span),
        present_extra_gains.reshape(attender_count, channel_span),
    )
    mixed = mixed_heads.reshape(seq_count, model_width).astype(jnp.bfloat16)
    new_state = memory_grid.reshape(seq_count, attender_count, channel_span * channel_span)
    partial_rows = jnp.dot(
        lax.all_gather(mixed, "ep", axis=0, tiled=True),
        result_map,
        preferred_element_type=jnp.float32,
    ).astype(jnp.bfloat16)
    mixer_out = lax.all_to_all(partial_rows, "ep", split_axis=0, concat_axis=1, tiled=True)
    residual = (latest_embeddings.astype(jnp.float32) + mixer_out.astype(jnp.float32)).astype(
        jnp.bfloat16
    )
    second = rms_norm(residual, later_rescale_gain)
    top_count = picked_specialists.shape[1]
    expert_count = specialist_switch_maps.shape[0] * devices
    group_size = expert_count // GROUPS
    capacity = ((seq_count + 1) // 2 * top_count + group_size - 1) // group_size
    flat_ids = picked_specialists.reshape(-1)
    matches = (flat_ids[:, None] == jnp.arange(expert_count, dtype=jnp.int32)[None, :]).astype(
        jnp.int32
    )
    slot_rank = jnp.sum((jnp.cumsum(matches, axis=0) - matches) * matches, axis=1)
    slot_ids = flat_ids * capacity + slot_rank
    picks = (
        slot_ids[:, None] == jnp.arange(expert_count * capacity, dtype=jnp.int32)[None, :]
    ).astype(jnp.bfloat16)
    repeated = jnp.repeat(second, top_count, axis=0)
    send_rows = jnp.einsum("sk,sd->kd", picks, repeated, preferred_element_type=jnp.float32).astype(
        jnp.bfloat16
    )
    send_rows = send_rows.reshape(devices, expert_count // devices * capacity, model_width)
    received = lax.all_to_all(send_rows, "ep", split_axis=0, concat_axis=0, tiled=True)
    rows_in = received.reshape(-1, model_width)
    gate_proj = jnp.dot(rows_in, specialist_switch_maps[0], preferred_element_type=jnp.float32)
    up_proj = jnp.dot(rows_in, specialist_widen_maps[0], preferred_element_type=jnp.float32)
    hidden_act = (jax.nn.silu(gate_proj) * up_proj).astype(jnp.bfloat16)
    results = jnp.dot(
        hidden_act, specialist_shrink_maps[0], preferred_element_type=jnp.float32
    ).astype(jnp.bfloat16)
    returned = lax.all_to_all(
        results.reshape(received.shape), "ep", split_axis=0, concat_axis=0, tiled=True
    )
    collected = jnp.dot(
        picks, returned.reshape(-1, model_width), preferred_element_type=jnp.float32
    )
    expert_sum = jnp.sum(
        collected.reshape(seq_count, top_count, model_width) * specialist_picked_shares[:, :, None],
        axis=1,
    )
    new_hidden = (residual.astype(jnp.float32) + expert_sum).astype(jnp.bfloat16)
    return (new_hidden, new_state)


def step(*args):
    devices, columns = lax.axis_size("ep"), args[3].shape[1]
    if devices % (2 * GROUPS) == 0 and (2 * columns) % 128 == 0 and args[18].shape[0] == 1:
        return layered(*args)
    return local(*args)


def solution(mesh):
    return jax.shard_map(
        step,
        mesh=mesh,
        in_specs=(
            P("ep", None),
            P("ep", None, None),
            P(),
            P(None, "ep"),
            P(None, "ep"),
            P(None, "ep"),
            P(),
            P(),
            P(),
            P(),
            P(),
            P(),
            P(),
            P(),
            P(),
            P(),
            P(None, "ep"),
            P(),
            P("ep", None, None),
            P("ep", None, None),
            P("ep", None, None),
            P("ep", None),
            P("ep", None),
        ),
        out_specs=(P("ep", None), P("ep", None, None)),
        check_vma=False,
    )
```

```python
import functools
import math

import jax
import jax.numpy as jnp
from jax import lax
from jax.experimental import pallas as pl
from jax.experimental.pallas import tpu as pltpu
from jax.sharding import PartitionSpec as P


GROUPS = 4


norm_eps = 1e-06
group_eps = 0.00064
unit_eps = 1e-06

f32 = jnp.float32
bf16 = jnp.bfloat16


def rms_rows(values, gain):
    scale = lax.rsqrt(jnp.mean(values * values, axis=-1, keepdims=True) + norm_eps)
    return (values * scale * gain).astype(bf16)


def split_dot(values, selector):
    high = values.astype(bf16)
    low = (values - high.astype(f32)).astype(bf16)
    return jnp.dot(high, selector, preferred_element_type=f32) + jnp.dot(
        low, selector, preferred_element_type=f32
    )


def turned_dot(rows, columns):
    return lax.dot_general(rows, columns, (((1,), (1,)), ((), ())), preferred_element_type=f32)


def project_kernel(chips, where_ref, *refs):
    rows_refs, (gain_ref, *map_refs, out_ref, maps) = refs[:chips], refs[chips:]
    plane, place, core = where_ref[0], where_ref[1], where_ref[2]
    own_refs, pair_refs = map_refs[:3], map_refs[3:]
    columns = own_refs[0].shape[0]

    def lay(lower_refs, upper_refs):
        for m in range(3):
            maps[2 * m * columns : (2 * m + 1) * columns, :] = lower_refs[m][...]
            maps[(2 * m + 1) * columns : (2 * m + 2) * columns, :] = upper_refs[m][...]

    pl.when(core == 0)(lambda: lay(own_refs, pair_refs))
    pl.when(core != 0)(lambda: lay(pair_refs, own_refs))
    normed = jnp.concatenate(
        [rms_rows(ref[...].astype(f32), gain_ref[...]) for ref in rows_refs], axis=0
    )
    result = turned_dot(normed, maps[...]).astype(bf16)
    seqs = result.shape[0] // (GROUPS * chips)
    for kp in range(chips):
        for kz in range(GROUPS):
            chip = (plane ^ kz) * chips + (place ^ kp)
            block = (kp * GROUPS + kz) * seqs
            out_ref[pl.ds(pl.multiple_of(chip * seqs, seqs), seqs), :] = result[
                block : block + seqs
            ]


def state_kernel(
    channel,
    lanes,
    arrived_ref,
    decay_ref,
    rate_ref,
    tail_ref,
    erase_ref,
    substitute_ref,
    extra_ref,
    attend_ref,
    state_ref,
    new_ref,
    mixed_ref,
    memory,
    erase2,
    write2,
    replace2,
    query2,
    decay2,
    value2,
    spare,
    values,
    readout,
    in_sems,
    out_sems,
):
    seqs, heads, width = memory.shape
    rows = seqs * heads
    span = 256
    tile = 2 * channel
    chunks = width // lanes
    parts = lanes // span

    def copy_in(c):
        at = pl.ds(pl.multiple_of(c * lanes, lanes), lanes)
        return pltpu.make_async_copy(state_ref.at[:, :, at], memory.at[:, :, at], in_sems.at[c])

    def copy_out(c):
        at = pl.ds(pl.multiple_of(c * lanes, lanes), lanes)
        return pltpu.make_async_copy(memory.at[:, :, at], new_ref.at[:, :, at], out_sems.at[c])

    for c in range(chunks):
        copy_in(c).start()

    lower = lax.broadcasted_iota(jnp.int32, (seqs, tile), 1) < channel

    def lay(target, block, pair):
        turned = pltpu.roll(block, channel, 1)
        target[pl.ds(2 * pair, seqs, stride=heads), :] = jnp.where(lower, block, turned)
        target[pl.ds(2 * pair + 1, seqs, stride=heads), :] = jnp.where(lower, turned, block)

    for pair in range(heads // 2):
        block = arrived_ref[pair * seqs : (pair + 1) * seqs, :].astype(f32)
        for m, target in enumerate((query2, replace2, value2)):
            lay(target, block[:, m * tile : (m + 1) * tile], pair)
        lay(decay2, decay_ref[:, pair * tile : (pair + 1) * tile], pair)
        lay(spare, rate_ref[:, pair * tile : (pair + 1) * tile], pair)

    def over_rows(ref):
        return jnp.broadcast_to(ref[...][None], (seqs, heads, tile)).reshape(rows, tile)

    def head_sum(x):
        return 0.5 * jnp.sum(x, axis=-1, keepdims=True)

    key, rate = replace2[...], spare[...]
    erase = key * over_rows(erase_ref)
    erase = erase * lax.rsqrt(head_sum(erase * erase) + unit_eps)
    erase2[...] = erase
    write2[...] = erase * rate
    replace = key * (1.0 + (rate - 1.0) * over_rows(substitute_ref))
    replace2[...] = replace
    spare[...] = head_sum(query2[...] * replace * over_rows(extra_ref)) * value2[...]
    values[...] = value2[:, :channel].astype(bf16)
    readout[...] = jnp.zeros_like(readout)

    def wide(ref):
        return jnp.concatenate([ref[...]] * (span // tile), axis=-1)

    def iota(shape, axis):
        return lax.broadcasted_iota(jnp.int32, shape, axis)

    def mask(chosen):
        return chosen.astype(f32).astype(bf16)

    block_ones = mask(iota((span, span), 0) // channel == iota((span, span), 1) // channel)

    def chunk(c, carry):
        copy_in(c).wait()
        for part in range(parts):
            at = pl.multiple_of(c * lanes + part * span, span)
            first = at // channel
            spread = mask(
                iota((channel, span), 0) == iota((channel, span), 1) // channel + first
            )
            collect = mask(
                iota((span, channel), 0) // channel + first == iota((span, channel), 1)
            )
            grid = memory[:, :, pl.ds(at, span)].reshape(rows, span)
            removed = jnp.dot(
                (grid * wide(erase2)).astype(bf16), block_ones, preferred_element_type=f32
            )
            value_wide = jnp.dot(values[...], spread, preferred_element_type=f32)
            grid = grid * wide(decay2) - removed * wide(write2) + value_wide * wide(replace2)
            memory[:, :, pl.ds(at, span)] = grid.reshape(seqs, heads, span)
            readout[...] += split_dot(grid * wide(query2), collect)
        copy_out(c).start()
        return carry

    lax.fori_loop(0, chunks, chunk, 0)

    result = readout[...]
    centered = result - jnp.mean(result, axis=-1, keepdims=True)
    variance = jnp.mean(centered * centered, axis=-1, keepdims=True)
    gain = over_rows(attend_ref)[:, :channel]
    mixed = centered * lax.rsqrt(variance + group_eps) * gain + spare[:, :channel]
    spare[:, :channel] = mixed
    for pair in range(heads // 2):
        left = spare[pl.ds(2 * pair, seqs, stride=heads), :]
        right = spare[pl.ds(2 * pair + 1, seqs, stride=heads), :]
        mixed_ref[:, pair * tile : (pair + 1) * tile] = jnp.where(
            lower, left, pltpu.roll(right, channel, 1)
        ).astype(bf16)
    mixed_ref[:, heads * channel :] = tail_ref[...]
    for c in range(chunks):
        copy_out(c).wait()


def output_kernel(room, members, chips, where_ref, *refs):
    mixed_refs, own_ref, refs = refs[:GROUPS], refs[GROUPS], refs[GROUPS + 1 :]
    others = chips - 1
    near_refs, far_refs, refs = refs[:others], refs[others : 2 * others], refs[2 * others :]
    part_refs, (pick_ref, tail_ref, mixed, result) = refs[:GROUPS], refs[GROUPS:]
    plane, place, core = where_ref[0], where_ref[1], where_ref[2]
    columns, depth = own_ref.shape
    half = depth // 2
    seqs = mixed_refs[0].shape[0]
    rows = GROUPS * seqs
    for k, ref in enumerate(mixed_refs):
        mixed[k * seqs : (k + 1) * seqs, :] = ref[...]
    near = mixed[:, pl.ds(pl.multiple_of(core * half, half), half)]
    far = mixed[:, pl.ds(pl.multiple_of((1 - core) * half, half), half)]
    for kp in range(chips):
        if kp == 0:
            block = turned_dot(mixed[:, :depth], own_ref[...])
        else:
            block = turned_dot(near, near_refs[kp - 1][...]) + turned_dot(
                far, far_refs[kp - 1][...]
            )
        at = pl.multiple_of((place ^ kp) * columns, columns)
        result[:, pl.ds(at, columns)] = block.astype(bf16)

    def iota(shape, axis):
        return lax.broadcasted_iota(jnp.int32, shape, axis)

    tail = mixed[:, depth:]
    at = iota(tail.shape, 1) == 2 * members
    group = jnp.sum(jnp.where(at, tail.astype(f32), 0.0), axis=1, keepdims=True)
    above, along = iota((rows, rows), 0), iota((rows, rows), 1)
    group_row = jnp.sum(jnp.where(above == along, group, 0.0), axis=0, keepdims=True)
    earlier = (above // seqs == along // seqs) & (above < along) & (group == group_row)
    rank = jnp.sum(earlier.astype(f32), axis=0, keepdims=True)
    slot, lane = iota((GROUPS * room, rows), 0), iota((GROUPS * room, rows), 1)
    for k, part_ref in enumerate(part_refs):
        pick = (
            (lane // seqs == ((slot // room) ^ k))
            & (group_row == (plane ^ k).astype(f32))
            & (rank == (slot % room).astype(f32))
        )
        pick = pick.astype(f32).astype(bf16)
        part_ref[...] = jnp.dot(pick, result[...], preferred_element_type=f32).astype(bf16)
        if k == 0:
            pick_ref[...] = pick
            tail_ref[...] = jnp.dot(pick, tail, preferred_element_type=f32).astype(bf16)


def residual_kernel(where_ref, *refs):
    parts, (rows_ref, tail_ref, gain_ref, chosen_ref, residual_ref, held) = (
        refs[:GROUPS],
        refs[GROUPS:],
    )
    plane = where_ref[0]
    width = rows_ref.shape[1]
    columns = width // GROUPS
    for k, part_ref in enumerate(parts):
        at = pl.multiple_of((plane ^ k) * columns, columns)
        held[:, pl.ds(at, columns)] = rows_ref[:, pl.ds(at, columns)].astype(f32) + part_ref[
            ...
        ].astype(f32)
    residual = held[...].astype(bf16)
    residual_ref[...] = residual
    chosen_ref[:, :width] = rms_rows(residual.astype(f32), gain_ref[...])
    chosen_ref[:, width:] = tail_ref[...]


def expert_kernel(members, where_ref, *refs):
    blocks, (switch_ref, widen_ref, shrink_ref, mine_ref, theirs_ref, rows) = (
        refs[:members],
        refs[members:],
    )
    width = switch_ref.shape[1]
    size = blocks[0].shape[0]
    for i, ref in enumerate(blocks):
        rows[i * size : (i + 1) * size, :] = ref[...]
    tokens = rows[:, :width]
    gate = jnp.dot(tokens, switch_ref[0], preferred_element_type=f32)
    up = jnp.dot(tokens, widen_ref[0], preferred_element_type=f32)
    hidden = (gate * jax.nn.sigmoid(gate) * up).astype(bf16)
    tail = rows[:, width:].astype(f32)
    lane = lax.broadcasted_iota(jnp.int32, tail.shape, 1)
    member = where_ref[3]
    share = jnp.sum(
        jnp.where((lane == member) | (lane == member + members), tail, 0.0), axis=-1, keepdims=True
    )
    result = jnp.dot(hidden, shrink_ref[0], preferred_element_type=f32) * share
    half = result.shape[0] // 2
    mine_ref[...] = result[:half].astype(bf16)
    theirs_ref[...] = result[half:].astype(bf16)


def swap(rows, mask):
    count = lax.axis_size("ep")
    return lax.ppermute(rows, "ep", [(i, i ^ mask) for i in range(count)])


def layered(
    latest_embeddings,
    prior_memory_grids,
    earlier_rescale_gain,
    query_map,
    lookup_map,
    content_map,
    forget_lower_map,
    forget_upper_map,
    forget_shift,
    adapt_lower_map,
    adapt_upper_map,
    adapt_shift,
    erase_lookup_gains,
    substitute_lookup_gains,
    present_extra_gains,
    attender_rescale_gain,
    result_map,
    later_rescale_gain,
    specialist_switch_maps,
    specialist_widen_maps,
    specialist_shrink_maps,
    picked_specialists,
    specialist_picked_shares,
):
    seqs, width = latest_embeddings.shape
    heads = prior_memory_grids.shape[1]
    channel = width // heads
    devices = lax.axis_size("ep")
    members = devices // GROUPS
    chips = members // 2
    columns = query_map.shape[1]
    me = lax.axis_index("ep").astype(jnp.int32)
    core, place, plane = me % 2, (me // 2) % chips, me // members
    where = jnp.stack([plane, place, core, me % members])
    smem = pl.BlockSpec(memory_space=pltpu.SMEM)
    vmem = pl.BlockSpec(memory_space=pltpu.VMEM)
    same_core = [[2 * i + c for i in range(devices // 2)] for c in range(2)]

    def limit(mib):
        return pltpu.CompilerParams(vmem_limit_bytes=mib * 2**20)

    line = [latest_embeddings] + [swap(latest_embeddings, members * k) for k in range(1, GROUPS)]
    line_rows = jnp.concatenate(line, axis=0)
    gathered = [line_rows] + [swap(line_rows, 2 * k) for k in range(1, chips)]

    own_maps = [m.T for m in (query_map, lookup_map, content_map, result_map)]
    pair_maps = [swap(m, 1) for m in own_maps]

    late_rows, late_picks, late_shares, _ = lax.optimization_barrier(
        (latest_embeddings, picked_specialists, specialist_picked_shares, line_rows)
    )
    normed = rms_rows(late_rows.astype(f32), earlier_rescale_gain)
    decay_low = jnp.tanh(
        jnp.dot(normed, forget_lower_map, preferred_element_type=f32)
    ).astype(bf16)
    decay = jnp.exp(
        -math.exp(-0.5)
        * jax.nn.sigmoid(
            forget_shift + jnp.dot(decay_low, forget_upper_map, preferred_element_type=f32)
        )
    )
    rate_low = jnp.dot(normed, adapt_lower_map, preferred_element_type=f32).astype(bf16)
    rate = jax.nn.sigmoid(
        adapt_shift + jnp.dot(rate_low, adapt_upper_map, preferred_element_type=f32)
    )

    group = late_picks[:, 0] // members
    share_at = (
        late_picks[:, :, None] % members == jnp.arange(members, dtype=jnp.int32)
    ).astype(f32)
    shares = jnp.sum(share_at * late_shares[:, :, None], axis=1)
    share_high = shares.astype(bf16)
    share_low = (shares - share_high.astype(f32)).astype(bf16)
    tail_width = -(-(2 * members + 1) // 128) * 128
    tail = jnp.concatenate(
        [
            share_high,
            share_low,
            group[:, None].astype(bf16),
            jnp.zeros((seqs, tail_width - 2 * members - 1), bf16),
        ],
        axis=1,
    )

    all_rows = seqs * GROUPS * chips
    projected = pl.pallas_call(
        functools.partial(project_kernel, chips),
        out_shape=jax.ShapeDtypeStruct((all_rows, 6 * columns), bf16),
        in_specs=[smem] + [vmem] * (chips + 7),
        out_specs=vmem,
        scratch_shapes=[pltpu.VMEM((6 * columns, width), bf16)],
        compiler_params=limit(16),
        name="project",
    )(where, *gathered, earlier_rescale_gain.reshape(1, width), *own_maps[:3], *pair_maps[:3])
    arrived = lax.all_to_all(
        projected, "ep", split_axis=0, concat_axis=0, tiled=True, axis_index_groups=same_core
    )
    chip_map = jnp.where(
        core == 0,
        jnp.concatenate([own_maps[3], pair_maps[3]], axis=0),
        jnp.concatenate([pair_maps[3], own_maps[3]], axis=0),
    )
    half = lax.dynamic_slice_in_dim(chip_map, core * (width // 2), width // 2, axis=1)
    half, _ = lax.optimization_barrier((half, projected))
    near = [swap(half, 2 * k) for k in range(1, chips)]

    lanes = 1024
    rows = seqs * heads

    def twice(gains):
        gains = gains.reshape(heads, channel)
        return jnp.concatenate([gains, gains], axis=1)

    hbm = pl.BlockSpec(memory_space=pltpu.HBM)
    tile = pltpu.VMEM((rows, 2 * channel), f32)
    sems = pltpu.SemaphoreType.DMA((channel * channel // lanes,))
    new_state, mixed_rows = pl.pallas_call(
        functools.partial(state_kernel, channel, lanes),
        out_shape=[
            jax.ShapeDtypeStruct(prior_memory_grids.shape, f32),
            jax.ShapeDtypeStruct((seqs, width + tail_width), bf16),
        ],
        in_specs=[vmem] * 8 + [hbm],
        out_specs=[hbm, vmem],
        scratch_shapes=[pltpu.VMEM(prior_memory_grids.shape, f32)]
        + [tile] * 7
        + [pltpu.VMEM((rows, channel), bf16), pltpu.VMEM((rows, channel), f32), sems, sems],
        compiler_params=limit(57),
        name="state",
    )(
        arrived,
        decay,
        rate,
        tail,
        twice(erase_lookup_gains),
        twice(substitute_lookup_gains),
        twice(present_extra_gains),
        twice(attender_rescale_gain),
        prior_memory_grids,
    )

    mixed_line = [mixed_rows] + [swap(mixed_rows, members * k) for k in range(1, GROUPS)]
    near, _ = lax.optimization_barrier((near, mixed_rows))
    far = [swap(part, 1) for part in near]
    room = (seqs + 1) // 2
    count = GROUPS * room
    *parts, pick, chosen_tail = pl.pallas_call(
        functools.partial(output_kernel, room, members, chips),
        out_shape=[jax.ShapeDtypeStruct((count, width // GROUPS), bf16)] * GROUPS
        + [
            jax.ShapeDtypeStruct((count, GROUPS * seqs), bf16),
            jax.ShapeDtypeStruct((count, tail_width), bf16),
        ],
        in_specs=[smem] + [vmem] * (GROUPS + 1 + 2 * (chips - 1)),
        out_specs=[vmem] * (GROUPS + 2),
        scratch_shapes=[
            pltpu.VMEM((GROUPS * seqs, width + tail_width), bf16),
            pltpu.VMEM((GROUPS * seqs, width // GROUPS), bf16),
        ],
        compiler_params=limit(16),
        name="output",
    )(where, *mixed_line, chip_map, *near, *far)
    parts = [parts[0]] + [swap(parts[k], members * k) for k in range(1, GROUPS)]
    chosen_rows = jnp.dot(pick, line_rows, preferred_element_type=f32).astype(bf16)
    chosen, residual = pl.pallas_call(
        residual_kernel,
        out_shape=[
            jax.ShapeDtypeStruct((count, width + tail_width), bf16),
            jax.ShapeDtypeStruct((count, width), bf16),
        ],
        in_specs=[smem] + [vmem] * (GROUPS + 3),
        out_specs=[vmem] * 2,
        scratch_shapes=[pltpu.VMEM((count, width), f32)],
        compiler_params=limit(8),
        name="residual",
    )(where, *parts, chosen_rows, chosen_tail, later_rescale_gain.reshape(1, width))

    own_rows = [chosen] + [swap(chosen, 2 * k) for k in range(1, chips)]
    other_rows = [swap(rows, 1) for rows in own_rows]
    mine, theirs = pl.pallas_call(
        functools.partial(expert_kernel, members),
        out_shape=[jax.ShapeDtypeStruct((chips * count, width), bf16)] * 2,
        in_specs=[smem] + [vmem] * (members + 3),
        out_specs=[vmem] * 2,
        scratch_shapes=[pltpu.VMEM((members * count, width + tail_width), bf16)],
        compiler_params=limit(24),
        name="expert",
    )(
        where,
        *own_rows,
        *other_rows,
        specialist_switch_maps,
        specialist_widen_maps,
        specialist_shrink_maps,
    )

    both = (mine.astype(f32) + swap(theirs, 1).astype(f32)).astype(bf16)
    pieces = [both[k * count : (k + 1) * count] for k in range(chips)]
    pieces = [pieces[0]] + [swap(pieces[k], 2 * k) for k in range(1, chips)]
    finished = residual.astype(f32)
    for piece in pieces:
        finished = finished + piece.astype(f32)
    finished = finished.astype(bf16).reshape(GROUPS, room, width)
    home = jnp.concatenate(
        [finished[0]] + [swap(finished[k], members * k) for k in range(1, GROUPS)], axis=0
    )
    earlier = (group[None, :] == group[:, None]) & (
        jnp.arange(seqs)[None, :] < jnp.arange(seqs)[:, None]
    )
    slot = (group ^ plane) * room + jnp.sum(earlier, axis=1).astype(jnp.int32)
    fetch = (slot[:, None] == jnp.arange(count, dtype=jnp.int32)[None, :]).astype(bf16)
    new_hidden = jnp.dot(fetch, home, preferred_element_type=f32).astype(bf16)
    return (new_hidden, new_state)


def rms_norm(rows_in, gain):
    values = rows_in.astype(jnp.float32)
    scale = lax.rsqrt(jnp.mean(values * values, axis=-1, keepdims=True) + norm_eps)
    return (values * scale * gain).astype(jnp.bfloat16)


def memory_readout(
    query_signal,
    substitute_lookup,
    content_signals,
    forget_multiplier,
    adapt_speed,
    erase_signal,
    memory_grid,
    attender_rescale_gain,
    present_extra_gains,
):
    highest = lax.Precision.HIGHEST
    removed = jnp.einsum("bhij,bhj->bhi", memory_grid, erase_signal, precision=highest)
    memory_grid = (
        memory_grid * forget_multiplier[:, :, None, :]
        - removed[..., None] * (erase_signal * adapt_speed)[:, :, None, :]
        + content_signals[..., None] * substitute_lookup[:, :, None, :]
    )
    readout = jnp.einsum("bhij,bhj->bhi", memory_grid, query_signal, precision=highest)
    centered = readout - jnp.mean(readout, axis=-1, keepdims=True)
    variance = jnp.mean(centered * centered, axis=-1, keepdims=True)
    rescaled_result = centered * lax.rsqrt(variance + group_eps) * attender_rescale_gain
    present_extra = (
        jnp.sum(query_signal * substitute_lookup * present_extra_gains, axis=-1, keepdims=True)
        * content_signals
    )
    return (rescaled_result + present_extra, memory_grid)


def local(
    latest_embeddings,
    prior_memory_grids,
    earlier_rescale_gain,
    query_map,
    lookup_map,
    content_map,
    forget_lower_map,
    forget_upper_map,
    forget_shift,
    adapt_lower_map,
    adapt_upper_map,
    adapt_shift,
    erase_lookup_gains,
    substitute_lookup_gains,
    present_extra_gains,
    attender_rescale_gain,
    result_map,
    later_rescale_gain,
    specialist_switch_maps,
    specialist_widen_maps,
    specialist_shrink_maps,
    picked_specialists,
    specialist_picked_shares,
):
    seq_count, model_width = latest_embeddings.shape
    attender_count = prior_memory_grids.shape[1]
    channel_span = model_width // attender_count
    devices = lax.axis_size("ep")
    columns = query_map.shape[1]
    normed = rms_norm(latest_embeddings, earlier_rescale_gain)
    stacked = jnp.concatenate([query_map, lookup_map, content_map], axis=1)
    projected = jnp.dot(
        lax.all_gather(normed, "ep", axis=0, tiled=True),
        stacked,
        preferred_element_type=jnp.float32,
    ).astype(jnp.bfloat16)
    query_signal, key_rows, content_signals = (
        lax.all_to_all(projected[:, :columns], "ep", split_axis=0, concat_axis=1, tiled=True),
        lax.all_to_all(
            projected[:, columns : 2 * columns], "ep", split_axis=0, concat_axis=1, tiled=True
        ),
        lax.all_to_all(projected[:, 2 * columns :], "ep", split_axis=0, concat_axis=1, tiled=True),
    )
    decay_low = jnp.tanh(
        jnp.dot(normed, forget_lower_map, preferred_element_type=jnp.float32)
    ).astype(jnp.bfloat16)
    forget_multiplier = jnp.exp(
        -math.exp(-0.5)
        * jax.nn.sigmoid(
            forget_shift + jnp.dot(decay_low, forget_upper_map, preferred_element_type=jnp.float32)
        )
    )
    rate_low = jnp.dot(normed, adapt_lower_map, preferred_element_type=jnp.float32).astype(
        jnp.bfloat16
    )
    adapt_speed = jax.nn.sigmoid(
        adapt_shift + jnp.dot(rate_low, adapt_upper_map, preferred_element_type=jnp.float32)
    )
    key_float = key_rows.astype(jnp.float32)
    erase_signal = (key_float * erase_lookup_gains).reshape(seq_count, attender_count, channel_span)
    erase_signal = erase_signal * lax.rsqrt(
        jnp.sum(erase_signal * erase_signal, axis=-1, keepdims=True) + unit_eps
    )
    substitute_lookup = key_float * (1.0 + (adapt_speed - 1.0) * substitute_lookup_gains)
    head_shape = (seq_count, attender_count, channel_span)
    mixed_heads, memory_grid = memory_readout(
        query_signal.astype(jnp.float32).reshape(head_shape),
        substitute_lookup.reshape(head_shape),
        content_signals.astype(jnp.float32).reshape(head_shape),
        forget_multiplier.reshape(head_shape),
        adapt_speed.reshape(head_shape),
        erase_signal,
        prior_memory_grids.reshape(seq_count, attender_count, channel_span, channel_span),
        attender_rescale_gain.reshape(attender_count, channel_span),
        present_extra_gains.reshape(attender_count, channel_span),
    )
    mixed = mixed_heads.reshape(seq_count, model_width).astype(jnp.bfloat16)
    new_state = memory_grid.reshape(seq_count, attender_count, channel_span * channel_span)
    partial_rows = jnp.dot(
        lax.all_gather(mixed, "ep", axis=0, tiled=True),
        result_map,
        preferred_element_type=jnp.float32,
    ).astype(jnp.bfloat16)
    mixer_out = lax.all_to_all(partial_rows, "ep", split_axis=0, concat_axis=1, tiled=True)
    residual = (latest_embeddings.astype(jnp.float32) + mixer_out.astype(jnp.float32)).astype(
        jnp.bfloat16
    )
    second = rms_norm(residual, later_rescale_gain)
    top_count = picked_specialists.shape[1]
    expert_count = specialist_switch_maps.shape[0] * devices
    group_size = expert_count // GROUPS
    capacity = ((seq_count + 1) // 2 * top_count + group_size - 1) // group_size
    flat_ids = picked_specialists.reshape(-1)
    matches = (flat_ids[:, None] == jnp.arange(expert_count, dtype=jnp.int32)[None, :]).astype(
        jnp.int32
    )
    slot_rank = jnp.sum((jnp.cumsum(matches, axis=0) - matches) * matches, axis=1)
    slot_ids = flat_ids * capacity + slot_rank
    picks = (
        slot_ids[:, None] == jnp.arange(expert_count * capacity, dtype=jnp.int32)[None, :]
    ).astype(jnp.bfloat16)
    repeated = jnp.repeat(second, top_count, axis=0)
    send_rows = jnp.einsum("sk,sd->kd", picks, repeated, preferred_element_type=jnp.float32).astype(
        jnp.bfloat16
    )
    send_rows = send_rows.reshape(devices, expert_count // devices * capacity, model_width)
    received = lax.all_to_all(send_rows, "ep", split_axis=0, concat_axis=0, tiled=True)
    rows_in = received.reshape(-1, model_width)
    gate_proj = jnp.dot(rows_in, specialist_switch_maps[0], preferred_element_type=jnp.float32)
    up_proj = jnp.dot(rows_in, specialist_widen_maps[0], preferred_element_type=jnp.float32)
    hidden_act = (jax.nn.silu(gate_proj) * up_proj).astype(jnp.bfloat16)
    results = jnp.dot(
        hidden_act, specialist_shrink_maps[0], preferred_element_type=jnp.float32
    ).astype(jnp.bfloat16)
    returned = lax.all_to_all(
        results.reshape(received.shape), "ep", split_axis=0, concat_axis=0, tiled=True
    )
    collected = jnp.dot(
        picks, returned.reshape(-1, model_width), preferred_element_type=jnp.float32
    )
    expert_sum = jnp.sum(
        collected.reshape(seq_count, top_count, model_width) * specialist_picked_shares[:, :, None],
        axis=1,
    )
    new_hidden = (residual.astype(jnp.float32) + expert_sum).astype(jnp.bfloat16)
    return (new_hidden, new_state)


def step(*args):
    devices, columns = lax.axis_size("ep"), args[3].shape[1]
    if devices % (2 * GROUPS) == 0 and (2 * columns) % 128 == 0 and args[18].shape[0] == 1:
        return layered(*args)
    return local(*args)


def solution(mesh):
    return jax.shard_map(
        step,
        mesh=mesh,
        in_specs=(
            P("ep", None),
            P("ep", None, None),
            P(),
            P(None, "ep"),
            P(None, "ep"),
            P(None, "ep"),
            P(),
            P(),
            P(),
            P(),
            P(),
            P(),
            P(),
            P(),
            P(),
            P(),
            P(None, "ep"),
            P(),
            P("ep", None, None),
            P("ep", None, None),
            P("ep", None, None),
            P("ep", None),
            P("ep", None),
        ),
        out_specs=(P("ep", None), P("ep", None, None)),
        check_vma=False,
    )
```
